128 devices in a mesh: sp: 16 (over z, x), tp: 8 (over y, core).
Axes of the slice: x: 4, y: 4, z: 4, core: 2. Of those that a mesh axis runs over, the one named last changes fastest.
Arguments:
- resid: bfloat16 [12288, 3072], P('sp', 'tp'), may hold values from -12 to 12
- query: bfloat16 [12288, 1536], P('sp', 'tp'), may hold values from -6 to 6
- keys: bfloat16 [12288, 1536], P('sp', 'tp'), may hold values from -6 to 6
- values: bfloat16 [12288, 1536], P('sp', 'tp'), may hold values from -6 to 6
- out_gate: bfloat16 [12288, 1536], P('sp', 'tp'), may hold values from -6 to 6
- in_gate: float32 [16, 12288], P('tp', 'sp'), may hold values from -6 to 110
- forget: float32 [16, 12288], P('tp', 'sp'), may hold values from -1 to 16
- doc_ids: int32 [12288], P('sp'), may hold values from 0 to 7, never falling along the last dimension, each value on 1 to 3072 neighbouring positions
- head_gain: float32 [1536], P('tp'), may hold values from 0.1 to 1.9
- w_out: bfloat16 [1536, 3072], P('tp'), may hold values from -0.15625 to 0.15625
- ffn_gain: float32 [3072], replicated, may hold values from 0.1 to 1.9
- w_gate: bfloat16 [3072, 8448], P('sp', 'tp'), may hold values from -0.109375 to 0.109375
- w_value: bfloat16 [3072, 8448], P('sp', 'tp'), may hold values from -0.109375 to 0.109375
- conv_taps: float32 [3, 8448], P(None, 'tp'), may hold values from -3.5 to 3.5
- w_down: bfloat16 [8448, 3072], P('tp', 'sp'), may hold values from -0.0625 to 0.0625
Outputs:
- layer_out: bfloat16 [12288, 3072], P('sp', 'tp')
The draws below stay inside these ranges and needn't reach their ends.
Inputs may be any that keep to these rules, and one draw needn't show every extreme that they name: `doc_ids`: document numbers never fall along the positions; each document is 1 to 3072 positions long.
All inputs are finite; a program needn't handle non-finite values.
Results may differ from the reference program's by a relative error of at most 0.02.
Values may be sent and summed in bfloat16 or wider, within the bound.
No kernel may reach another device: no remote copies, remote signals or barrier semaphores. Data moves between devices by JAX's collectives and lax.ppermute only.
A program may use at most 128 MiB of HBM per device.

```python
import math
import jax
import jax.numpy as jnp
import numpy as np
from jax import lax

D = 3072
H = 16
DH = 96
FF = 8448
BLOCK = 64
TAPS = 3
TOK_DEV = 768
TOKENS = 12288
DOCS = 8
N_TP = 8


def draw_resid(key, part):
    base = jnp.clip(jax.random.normal(key, (TOKENS, D), jnp.float32), -6.0, 6.0)
    phase = jax.random.uniform(jax.random.fold_in(key, 1), (), jnp.float32, 0.0, 6.2832)
    columns = jnp.arange(D, dtype=jnp.float32)
    scale = 0.35 * jnp.exp(0.6 * jnp.sin(6.2832 * columns / D + phase))
    return (base * scale).astype(jnp.bfloat16)


def draw_in_gate(key, part):
    base = jnp.clip(jax.random.normal(key, (H, TOKENS), jnp.float32), -6.0, 6.0)
    return base


def draw_forget(key, part):
    limit = 4
    quick = jax.random.randint(jax.random.fold_in(key, 1), (H, 1), 0, 8) < limit
    rate = jnp.where(quick, 1.0 / 40.0, 1.0 / (4.0 * TOK_DEV))
    factor = jnp.exp(jax.random.uniform(jax.random.fold_in(key, 2), (H, TOKENS // 128), jnp.float32, -1.05, 1.05))
    factor = jnp.repeat(factor, 128, axis=1)
    noise = 0.5 * jnp.clip(jax.random.normal(jax.random.fold_in(key, 3), (H, TOKENS), jnp.float32), -6.0, 6.0)
    return -jnp.log(rate * factor) + noise


def steps_of(stream_key, extent, cuts, least, top_value):
    def one(position, blocks):
        draws = jax.random.uniform(jax.random.fold_in(jax.random.fold_in(stream_key, 6), position), (blocks,), jnp.float32, least / len(cuts), top_value / len(cuts))
        return jnp.repeat(jnp.exp(draws), extent[position] // blocks).reshape((-1,) + (1,) * (len(extent) - position - 1))

    gain = one(*cuts[0])
    for cut in cuts[1:]:
        gain = gain * one(*cut)
    return gain


def length_profile(count, total, most, skew):
    loads = [(1 << 20) // math.isqrt(rank ** skew) + 1 for rank in range(2, count + 1)]
    spare, counts = total - most - (count - 1), [1] * (count - 1)
    while spare > 0:
        free = [i for i in range(count - 1) if counts[i] < most]
        mass, remaining = sum([loads[i] for i in free]), spare
        for i in free:
            addition = min(most - counts[i], max(1, remaining * loads[i] // mass), spare)
            counts[i] = counts[i] + addition
            spare = spare - addition
    return np.array([most] + counts)


def uneven(stream_key, amount, total, reach, skew):
    if amount == 2:
        one = jax.random.randint(stream_key, (), max(1, total - reach), min(reach, total - 1) + 1)
        return jnp.stack([one, total - one])
    sizes = jnp.asarray(length_profile(amount, total, reach, skew), jnp.int32)
    pairs = (amount - 1) // 2
    giver, taker = sizes[1:1 + 2 * pairs:2], sizes[2:2 + 2 * pairs:2]
    margin = jnp.minimum(giver - 1, reach - taker)
    moved = jax.random.randint(jax.random.fold_in(stream_key, 1), (pairs,), 0, 1 << 20) % (margin + 1)
    sizes = sizes.at[1:1 + 2 * pairs:2].set(giver - moved).at[2:2 + 2 * pairs:2].set(taker + moved)
    return sizes[jax.random.permutation(jax.random.fold_in(stream_key, 2), amount)]


def centred(rng, dims, scale, most, shards=(), held_as=jnp.bfloat16):
    gain = steps_of(rng, dims, shards, -0.22, 0.18) if shards else 1.0
    entries = jax.random.normal(rng, dims, jnp.float32) * scale * gain
    return jnp.minimum(jnp.maximum(entries, -most), most).astype(held_as)


def setup_inputs(seed: int = 0) -> dict:
    splits = jax.random.split(jax.random.key(seed), 16)
    return {
        "resid": draw_resid(jax.random.fold_in(splits[15], 71), 0),
        "query": centred(splits[1], (TOKENS, H * DH), 1.0, 6.0, ((0, 16), (1, 8))),
        "keys": centred(splits[2], (TOKENS, H * DH), 1.0, 6.0, ((0, 16), (1, 8))),
        "values": centred(splits[3], (TOKENS, H * DH), 1.0, 6.0, ((0, 16), (1, 8))),
        "out_gate": centred(splits[4], (TOKENS, H * DH), 1.0, 6.0, ((0, 16), (1, 8))),
        "in_gate": draw_in_gate(jax.random.fold_in(splits[15], 71), 0),
        "forget": draw_forget(jax.random.fold_in(splits[15], 71), 0),
        "doc_ids": jnp.searchsorted(jnp.cumsum(uneven(splits[7], DOCS, TOKENS, 4 * TOK_DEV, 0)), jnp.arange(TOKENS), side="right").astype(jnp.int32),
        "head_gain": jnp.clip(1.0 + 0.18 * jax.random.normal(splits[8], (H * DH,), jnp.float32), 0.1, 1.9),
        "w_out": centred(splits[9], (H * DH, D), (H * DH) ** -0.5, 0.15625, ((0, 8),)),
        "ffn_gain": jnp.clip(1.0 + 0.18 * jax.random.normal(splits[10], (D,), jnp.float32), 0.1, 1.9),
        "w_gate": centred(splits[11], (D, FF), D ** -0.5, 0.109375, ((0, 16), (1, 8))),
        "w_value": centred(splits[12], (D, FF), D ** -0.5, 0.109375, ((0, 16), (1, 8))),
        "conv_taps": centred(splits[13], (TAPS, FF), TAPS ** -0.5, 3.5, ((1, 8),), jnp.float32),
        "w_down": centred(splits[14], (FF, D), FF ** -0.5, 0.0625, ((0, 8), (1, 16))),
    }


ABSENT = -1e+30
epsilon = 1e-06
head_floor = 1.0
HIGHEST = lax.Precision.HIGHEST

def combine(early, late):
    state_early, peak_early, decay_early, first_early, last_early, second_early = early
    state_late, peak_late, decay_late, first_late, last_late, second_late = late
    early_empty = last_early < 0.0
    late_empty = first_late < 0.0
    cut = (first_late != last_early) & jnp.logical_not(early_empty) & jnp.logical_not(late_empty)
    passed = jnp.where(cut, ABSENT, decay_late)
    peak = jnp.maximum(passed + peak_early, peak_late)
    keep = jnp.exp(passed + peak_early - peak)
    fresh = jnp.exp(peak_late - peak)
    state = keep[..., None, None] * state_early + fresh[..., None, None] * state_late
    return (state, peak, decay_early + passed, jnp.where(early_empty, first_late, first_early), jnp.where(late_empty, last_early, last_late), jnp.where(late_empty, second_early, second_late))

def empty_state(heads, width):
    return (jnp.zeros((heads, width, width), jnp.float32), jnp.full((heads,), ABSENT, jnp.float32), jnp.zeros((heads,), jnp.float32), jnp.full((1,), -1.0, jnp.float32), jnp.full((1,), -1.0, jnp.float32), jnp.full((1,), -1.0, jnp.float32))

def advance(carry, item):
    return (combine(carry, item), carry)

def block_parts(query, keys, values, in_gate, forget, seg):
    length, heads, width = query.shape
    count = length // BLOCK
    query_blocks = query.reshape(count, BLOCK, heads, width)
    key_blocks = (keys * width ** (-0.5)).reshape(count, BLOCK, heads, width)
    value_blocks = values.reshape(count, BLOCK, heads, width)
    gate_in = in_gate.T.reshape(count, BLOCK, heads)
    cumul = jnp.cumsum(jax.nn.log_sigmoid(forget.T).reshape(count, BLOCK, heads), axis=1)
    seg_blocks = seg.reshape(count, BLOCK)
    total = cumul[:, -1]
    in_last = (seg_blocks == seg_blocks[:, -1:])[:, :, None]
    weight_log = jnp.where(in_last, total[:, None] - cumul + gate_in, ABSENT)
    local_peak = lax.optimization_barrier(jnp.max(weight_log, axis=1))
    weights = jnp.exp(weight_log - local_peak[:, None])
    update = jnp.einsum('nchk,nchv->nhkv', weights[..., None] * key_blocks, value_blocks, precision=HIGHEST)
    whole = jnp.all(seg_blocks == seg_blocks[:, :1], axis=1)[:, None]
    decay = jnp.where(whole, total, ABSENT)
    elements = (update, local_peak, decay, seg_blocks[:, :1], seg_blocks[:, -1:], seg_blocks[:, -2:-1])
    return (elements, (query_blocks, key_blocks, value_blocks, gate_in, cumul, seg_blocks))

def block_outputs(before, parts):
    state, peak_prev, _, _, last_prev, _ = before
    query_blocks, key_blocks, value_blocks, gate_in, cumul, seg_blocks = parts
    count, span, heads, width = query_blocks.shape
    carried = (seg_blocks == last_prev)[:, :, None]
    inter = jnp.where(carried, cumul + peak_prev[:, None], ABSENT)
    places = jnp.arange(span)
    causal = (places[:, None] >= places[None, :])[None, :, :, None]
    same = (seg_blocks[:, :, None] == seg_blocks[:, None, :])[..., None]
    diff_log = jnp.where(causal & same, cumul[:, :, None] - cumul[:, None] + gate_in[:, None], ABSENT)
    top = jnp.maximum(inter, lax.optimization_barrier(jnp.max(diff_log, axis=2)))
    scores = jnp.einsum('nthd,nshd->ntsh', query_blocks, key_blocks, precision=HIGHEST) * jnp.exp(diff_log - top[:, :, None])
    result = jnp.einsum('ntsh,nshd->nthd', scores, value_blocks, precision=HIGHEST)
    result = result + jnp.exp(inter - top)[..., None] * jnp.einsum('nthk,nhkv->nthv', query_blocks, state, precision=HIGHEST)
    return result.reshape(count * span, heads, width)

def reference(resid, query, keys, values, out_gate, in_gate, forget, doc_ids, head_gain, w_out, ffn_gain, w_gate, w_value, conv_taps, w_down):
    length = query.shape[0]
    seg = doc_ids.astype(jnp.float32)
    query_f = query.astype(jnp.float32).reshape(length, H, DH)
    keys_f = keys.astype(jnp.float32).reshape(length, H, DH)
    values_f = values.astype(jnp.float32).reshape(length, H, DH)
    elements, parts = block_parts(query_f, keys_f, values_f, in_gate, forget, seg)
    _, before = lax.scan(advance, empty_state(H, DH), elements)
    memory_out = block_outputs(before, parts)
    normed = memory_out * lax.rsqrt(lax.optimization_barrier(jnp.mean(memory_out * memory_out, axis=-1, keepdims=True)) + head_floor)
    normed = normed.reshape(length, H * DH) * head_gain * jax.nn.sigmoid(out_gate.astype(jnp.float32))
    mix = normed.astype(jnp.bfloat16)
    width_group = H // N_TP * DH
    attended = jnp.zeros((length, D), jnp.float32)
    for index in range(N_TP):
        share = jnp.dot(mix[:, index * width_group:(index + 1) * width_group], w_out[index * width_group:(index + 1) * width_group], preferred_element_type=jnp.float32).astype(jnp.bfloat16)
        attended = attended + lax.optimization_barrier(share).astype(jnp.float32)
    residual_one = resid.astype(jnp.float32) + attended
    scale = lax.rsqrt(lax.optimization_barrier(jnp.mean(residual_one * residual_one, axis=1, keepdims=True)) + epsilon)
    normed_rows = (residual_one * scale * ffn_gain).astype(jnp.bfloat16)
    gate = jnp.dot(normed_rows, w_gate, preferred_element_type=jnp.float32).astype(jnp.bfloat16)
    value = jnp.dot(normed_rows, w_value, preferred_element_type=jnp.float32).astype(jnp.bfloat16)
    extended = jnp.concatenate([jnp.zeros((2, FF), jnp.bfloat16), gate], axis=0).astype(jnp.float32)
    ids = jnp.concatenate([jnp.full((2,), -1.0, jnp.float32), seg])
    near = (ids[1:-1] == seg)[:, None]
    far = (ids[:-2] == seg)[:, None]
    conv = conv_taps[2] * extended[2:] + conv_taps[1] * jnp.where(near, extended[1:-1], 0.0) + conv_taps[0] * jnp.where(far, extended[:-2], 0.0)
    hidden = (jax.nn.silu(conv) * value.astype(jnp.float32)).astype(jnp.bfloat16)
    group = FF // N_TP
    down = jnp.zeros((length, D), jnp.float32)
    for index in range(N_TP):
        partial_rows = jnp.dot(hidden[:, index * group:(index + 1) * group], w_down[index * group:(index + 1) * group], preferred_element_type=jnp.float32).astype(jnp.bfloat16)
        down = down + lax.optimization_barrier(partial_rows).astype(jnp.float32)
    return (residual_one + down).astype(jnp.bfloat16)
```

```python
import jax
import jax.numpy as jnp
from jax import lax
from jax.experimental import pallas as pl
from jax.experimental.pallas import tpu as pltpu
from jax.sharding import Mesh
from jax.sharding import PartitionSpec as P

DH = 96
DOC_MAX = 3072
SP = ("z", "x")
ABSENT = -1e30
EPS = 1e-06
HEAD_FLOOR = 1.0
F32 = jnp.float32
BF16 = jnp.bfloat16


def in_first_head(shape):
    return lax.broadcasted_iota(jnp.int32, shape, len(shape) - 1) < DH


def state_kernel(k_ref, v_ref, in_ref, forget_ref, doc_ref, pay_ref, row_ref, col_ref, scr):
    tokens, width = k_ref.shape
    lane = lax.broadcasted_iota(jnp.int32, (8, tokens), 1)
    doc = jnp.broadcast_to(doc_ref[...].astype(F32), (8, tokens))
    scr[...] = jnp.zeros_like(scr)
    scr[0:2, :] = forget_ref[...]
    raw = scr[...]
    total = jnp.minimum(raw, 0.0) - jnp.log1p(jnp.exp(-jnp.abs(raw)))
    step = 1
    while step < tokens:
        total = total + jnp.where(lane >= step, pltpu.roll(total, step, 1), 0.0)
        step *= 2
    scr[0:2, :] = in_ref[...]
    rest = scr[...] - total
    peak = rest
    step = 1
    while step < tokens:
        near = (lane >= step) & (pltpu.roll(doc, step, 1) == doc)
        peak = jnp.maximum(peak, jnp.where(near, pltpu.roll(peak, step, 1), ABSENT))
        step *= 2
    end_doc = doc[:, tokens - 1 : tokens]
    end_peak = peak[:, tokens - 1 : tokens]
    end_total = total[:, tokens - 1 : tokens]
    weight = jnp.where(doc == end_doc, jnp.exp(jnp.minimum(rest - end_peak, 0.0)), 0.0)
    row_ref[...] = jnp.zeros_like(row_ref)
    row_ref[0:2, :] = total[0:2, :]
    row_ref[2:4, :] = peak[0:2, :]
    row_ref[4:6, :] = weight[0:2, :]
    row_ref[6:7, :] = doc[0:1, :]
    scr[...] = row_ref[...]
    cols = scr[...].T
    col_ref[...] = cols
    row_ref[4:6, :] = rest[0:2, :]
    first = in_first_head((tokens, width))
    spread = jnp.where(first, cols[:, 4:5], cols[:, 5:6])
    weighted = (k_ref[...].astype(F32) * (spread * DH**-0.5)).astype(BF16)
    state = lax.dot_general(
        weighted, v_ref[...], (((0,), (0,)), ((), ())), preferred_element_type=F32
    )
    small = in_first_head((DH, width))
    pay_ref[0:DH, :] = jnp.where(small, state[0:DH, :], state[DH:, :]).astype(BF16)

    line = in_first_head((1, width))

    def spread_heads(x):
        return jnp.where(line, x[0:1, :], x[1:2, :])

    def split(x):
        high = x.astype(BF16).astype(F32)
        mid = (x - high).astype(BF16).astype(F32)
        return high, mid, x - high - mid

    lines = [
        *split(spread_heads(end_total + end_peak)),
        *split(spread_heads(end_total)),
        jnp.broadcast_to(end_doc[0:1, :] + 1.0, (1, width)),
        jnp.broadcast_to(doc[0:1, tokens - 2 : tokens - 1] + 1.0, (1, width)),
    ]
    place = lax.broadcasted_iota(jnp.int32, (16, width), 0)
    table = jnp.zeros((16, width), F32)
    for k, value in enumerate(lines):
        table = jnp.where(place == k, value, table)
    pay_ref[DH:, :] = table.astype(BF16)


def local_kernel(q_ref, k_ref, v_ref, row_ref, col_ref, out_ref):
    tokens, width = q_ref.shape
    block = 256
    for start in range(0, tokens, block):
        stop = start + block
        keys = k_ref[0:stop, :]
        vals = v_ref[0:stop, :]
        q = q_ref[start:stop, :]
        first = in_first_head((block, width))
        at = lax.broadcasted_iota(jnp.int32, (block, stop), 0) + start
        source = lax.broadcasted_iota(jnp.int32, (block, stop), 1)
        seen = (at >= source) & (row_ref[6:7, 0:stop] == col_ref[start:stop, 6:7])
        found = []
        for h in range(2):
            mine = jnp.where(first if h == 0 else jnp.logical_not(first), q, jnp.zeros_like(q))
            scores = lax.dot_general(
                mine, keys, (((1,), (1,)), ((), ())), preferred_element_type=F32
            )
            gap = row_ref[4 + h : 5 + h, 0:stop] - col_ref[start:stop, 2 + h : 3 + h]
            part = (scores * jnp.exp(jnp.where(seen, gap, ABSENT))).astype(BF16)
            found.append(jnp.dot(part, vals, preferred_element_type=F32))
        out_ref[start:stop, :] = jnp.where(first, found[0], found[1])


def mix_kernel(
    q_ref, gate_ref, local_ref, row_ref, col_ref, gain_ref, w_ref, *refs
):
    pays, (out_ref, ids_ref, mix_ref) = refs[:-3], refs[-3:]
    tokens, width = q_ref.shape

    @pl.when(pl.program_id(0) == 0)
    def _():
        own = row_ref[6:7, 0:1] + 1.0
        behind = jnp.zeros((1, width), F32)
        peaks, goods = [], []
        for ref in pays:
            table = ref[DH:, :].astype(F32)
            good = table[6:7, :] == own
            peaks.append(
                jnp.where(good, table[0:1, :] + table[1:2, :] + table[2:3, :] + behind, ABSENT)
            )
            goods.append(good)
            behind = behind + (table[3:4, :] + table[4:5, :] + table[5:6, :])
        best = peaks[0]
        for value in peaks[1:]:
            best = jnp.maximum(best, value)
        state = jnp.zeros((DH, width), F32)
        for ref, value, good in zip(pays, peaks, goods):
            state = state + jnp.where(good, jnp.exp(value - best), 0.0) * ref[0:DH, :].astype(F32)
        small = in_first_head((DH, width))
        whole = jnp.concatenate(
            [jnp.where(small, state, 0.0), jnp.where(small, 0.0, state)], axis=0
        ).astype(BF16)
        carried = jnp.dot(q_ref[...], whole, preferred_element_type=F32)
        first = in_first_head((tokens, width))
        total = jnp.where(first, col_ref[:, 0:1], col_ref[:, 1:2])
        peak = total + jnp.where(first, col_ref[:, 2:3], col_ref[:, 3:4])
        inter = jnp.where(col_ref[:, 6:7] + 1.0 == own, total + best, ABSENT)
        top = jnp.maximum(peak, inter)
        memory = (
            jnp.exp(peak - top) * (local_ref[...] * DH**-0.5) + jnp.exp(inter - top) * carried
        )
        square = memory * memory
        mean_0 = jnp.sum(jnp.where(first, square, 0.0), axis=1, keepdims=True) / DH
        mean_1 = jnp.sum(jnp.where(first, 0.0, square), axis=1, keepdims=True) / DH
        norm = jnp.where(first, lax.rsqrt(mean_0 + HEAD_FLOOR), lax.rsqrt(mean_1 + HEAD_FLOOR))
        gate = gate_ref[...].astype(F32)
        mix_ref[...] = (memory * norm * gain_ref[...] * (1.0 / (1.0 + jnp.exp(-gate)))).astype(BF16)
        ids_ref[...] = pays[0][DH : DH + 16, 0:128].astype(F32)[0:16, :]

    out_ref[0] = jnp.dot(mix_ref[...], w_ref[...], preferred_element_type=F32).astype(BF16)


def proj_kernel(x_ref, gain_ref, wg_ref, wv_ref, wt_ref, gate_ref, value_ref, tail_ref, x_scr):
    parts, tokens, cols = x_ref.shape
    j = pl.program_id(0)

    @pl.when(j == 0)
    def _():
        def block(i, _):
            at = pl.multiple_of(i * 64, 64)
            rows = pl.ds(at, 64)
            square = jnp.zeros((64, cols), F32)
            for p in range(parts):
                r = x_ref[p, rows, :].astype(F32)
                square = square + r * r
            mean = jnp.sum(square, axis=1, keepdims=True) / (parts * cols)
            scale = lax.rsqrt(mean + EPS)
            for p in range(parts):
                r = x_ref[p, rows, :].astype(F32)
                x_scr[rows, p * cols : (p + 1) * cols] = (
                    r * scale * gain_ref[0:1, p * cols : (p + 1) * cols]
                ).astype(BF16)
            return 0

        lax.fori_loop(0, tokens // 64, block, 0)

    x = x_scr[...]
    gate = jnp.dot(x, wg_ref[...], preferred_element_type=F32).astype(BF16)
    gate_ref[...] = gate
    value_ref[...] = jnp.dot(x, wv_ref[...], preferred_element_type=F32).astype(BF16)

    @pl.when(j == pl.num_programs(0) - 1)
    def _():
        tail_ref[...] = jnp.dot(x_scr[...], wt_ref[...], preferred_element_type=F32).astype(BF16)


def down_kernel(
    gate_ref, value_ref, tail_ref, edge_ref, ids_ref, doc_ref, taps_ref, w_ref, wt_ref, out_ref, h_scr
):
    tokens, main = gate_ref.shape

    @pl.when(pl.program_id(0) == 0)
    def _():
        row = lax.broadcasted_iota(jnp.int32, (tokens, 1), 0)
        doc = doc_ref[:, 6:7] + 1.0
        last = ids_ref[6:7, 0:1]
        second = ids_ref[7:8, 0:1]
        one = jnp.where(row == 0, last, pltpu.roll(jnp.broadcast_to(doc, (tokens, 128)), 1, 0)[:, 0:1])
        two = jnp.where(
            row == 0,
            second,
            jnp.where(row == 1, last, pltpu.roll(jnp.broadcast_to(doc, (tokens, 128)), 2, 0)[:, 0:1]),
        )
        near = (one == doc).astype(F32)
        far = (two == doc).astype(F32)

        def finish(gate, value, edge, taps):
            prev_1 = jnp.where(row == 0, edge[7:8, :], pltpu.roll(gate, 1, 0))
            prev_2 = jnp.where(
                row == 0, edge[6:7, :], jnp.where(row == 1, edge[7:8, :], pltpu.roll(gate, 2, 0))
            )
            conv = taps[2:3, :] * gate + taps[1:2, :] * (near * prev_1) + taps[0:1, :] * (far * prev_2)
            return conv / (1.0 + jnp.exp(-conv)) * value

        for at in range(0, main, 128):
            cut = slice(at, at + 128)
            h_scr[:, cut] = finish(
                gate_ref[:, cut].astype(F32),
                value_ref[:, cut].astype(F32),
                edge_ref[:, cut].astype(F32),
                taps_ref[:, cut],
            ).astype(BF16)
        tail = tail_ref[...].astype(F32)
        lane = lax.broadcasted_iota(jnp.int32, (tokens, 128), 1)
        mine = (lane >= 64) & (lane < 96)
        gate = jnp.where(mine, pltpu.roll(tail, 64, 1), 0.0)
        value = jnp.where(mine, pltpu.roll(tail, 32, 1), 0.0)
        edge = pltpu.roll(edge_ref[:, main : main + 128].astype(F32), 64, 1)
        done = finish(gate, value, edge, taps_ref[:, main : main + 128])
        h_scr[:, main : main + 128] = jnp.where(mine, done, 0.0).astype(BF16)

    contract = (((1,), (1,)), ((), ()))
    for p in range(out_ref.shape[0]):
        cols = out_ref.shape[2]
        rows = slice(p * cols, (p + 1) * cols)
        out_ref[p] = (
            lax.dot_general(h_scr[:, 0:main], w_ref[rows, :], contract, preferred_element_type=F32)
            + lax.dot_general(h_scr[:, main:], wt_ref[rows, :], contract, preferred_element_type=F32)
        ).astype(BF16)


def shape(dims, dtype):
    return jax.ShapeDtypeStruct(dims, dtype)


def whole(dims):
    return pl.BlockSpec(dims, lambda *_: (0,) * len(dims))


def body(
    resid,
    query,
    keys,
    values,
    out_gate,
    in_gate,
    forget,
    doc_ids,
    head_gain,
    w_out,
    ffn_gain,
    w_gate,
    w_value,
    conv_taps,
    w_down,
):
    tokens, width = query.shape
    cols = resid.shape[1]
    parts = w_out.shape[1] // cols
    model = w_out.shape[1]
    hidden = w_gate.shape[1]
    main = hidden // 128 * 128
    spare = hidden - main
    down_t = w_down.T
    packed = jnp.concatenate(
        [
            w_gate[:, :main],
            w_value[:, :main],
            down_t[:, :main],
            w_gate[:, main:],
            w_value[:, main:],
            down_t[:, main:],
            jnp.zeros((w_gate.shape[0], 128 - 3 * spare), BF16),
        ],
        axis=1,
    )
    weights = lax.all_gather(packed, SP, axis=0, tiled=True)
    taps = jnp.concatenate(
        [
            conv_taps[:, :main],
            jnp.zeros((3, 2 * spare), F32),
            conv_taps[:, main:],
            jnp.zeros((3, 128 - 3 * spare), F32),
        ],
        axis=1,
    )

    pay, rows, cols_aux = pl.pallas_call(
        state_kernel,
        out_shape=(
            shape((DH + 16, width), BF16),
            shape((8, tokens), F32),
            shape((tokens, 8), F32),
        ),
        scratch_shapes=[pltpu.VMEM((8, tokens), F32)],
        name="state",
    )(keys, values, in_gate, forget, doc_ids.reshape(1, tokens))
    count = lax.axis_size(SP)
    reach = -(-(DOC_MAX - 1) // tokens)
    pays = [
        lax.ppermute(pay, SP, [(i, i + k) for i in range(count - k)]) for k in range(1, reach + 1)
    ]
    local = pl.pallas_call(
        local_kernel,
        out_shape=shape((tokens, width), F32),
        name="local",
    )(query, keys, values, rows, cols_aux)
    share, ids = pl.pallas_call(
        mix_kernel,
        grid=(parts,),
        in_specs=[
            whole((tokens, width)),
            whole((tokens, width)),
            whole((tokens, width)),
            whole((8, tokens)),
            whole((tokens, 8)),
            whole((1, width)),
            pl.BlockSpec((width, cols), lambda j: (0, j)),
            *[whole((DH + 16, width)) for _ in pays],
        ],
        out_specs=(
            pl.BlockSpec((1, tokens, cols), lambda j: (j, 0, 0)),
            whole((16, 128)),
        ),
        out_shape=(shape((parts, tokens, cols), BF16), shape((16, 128), F32)),
        scratch_shapes=[pltpu.VMEM((tokens, width), BF16)],
        name="mix",
    )(query, out_gate, local, rows, cols_aux, head_gain.reshape(1, width), w_out, *pays)
    attended = lax.psum_scatter(share, "tp", scatter_dimension=0, tiled=False)
    residual_own = resid.astype(F32) + attended.astype(F32)
    full = lax.all_gather(residual_own.astype(BF16), "tp", axis=0, tiled=False)

    step = 512
    lanes = main // step
    gate, value, tail = pl.pallas_call(
        proj_kernel,
        grid=(lanes,),
        in_specs=[
            whole((parts, tokens, cols)),
            whole((1, model)),
            pl.BlockSpec((model, step), lambda j: (0, j)),
            pl.BlockSpec((model, step), lambda j: (0, lanes + j)),
            pl.BlockSpec((model, 128), lambda j: (0, 3 * main // 128)),
        ],
        out_specs=(
            pl.BlockSpec((tokens, step), lambda j: (0, j)),
            pl.BlockSpec((tokens, step), lambda j: (0, j)),
            whole((tokens, 128)),
        ),
        out_shape=(
            shape((tokens, main), BF16),
            shape((tokens, main), BF16),
            shape((tokens, 128), BF16),
        ),
        scratch_shapes=[pltpu.VMEM((tokens, model), BF16)],
        compiler_params=pltpu.CompilerParams(vmem_limit_bytes=56 * 2**20),
        name="proj",
    )(full, ffn_gain.reshape(1, model), weights, weights, weights)
    edge = lax.ppermute(
        jnp.concatenate([gate[tokens - 8 :], tail[tokens - 8 :]], axis=1),
        SP,
        [(i, i + 1) for i in range(count - 1)],
    )
    pieces = 2
    terms = pl.pallas_call(
        down_kernel,
        grid=(parts // pieces,),
        in_specs=[
            whole((tokens, main)),
            whole((tokens, main)),
            whole((tokens, 128)),
            whole((8, main + 128)),
            whole((16, 128)),
            whole((tokens, 8)),
            whole((3, main + 128)),
            pl.BlockSpec((pieces * cols, main), lambda j: (j, 2)),
            pl.BlockSpec((pieces * cols, 128), lambda j: (j, 3 * main // 128)),
        ],
        out_specs=pl.BlockSpec((pieces, tokens, cols), lambda j: (j, 0, 0)),
        out_shape=shape((parts, tokens, cols), BF16),
        scratch_shapes=[pltpu.VMEM((tokens, main + 128), BF16)],
        compiler_params=pltpu.CompilerParams(vmem_limit_bytes=56 * 2**20),
        name="down",
    )(gate, value, tail, edge, ids, cols_aux, taps, weights, weights)
    down = lax.psum_scatter(terms, "tp", scatter_dimension=0, tiled=False)
    return (residual_own + down.astype(F32)).astype(BF16)


def solution(mesh):
    torus = Mesh(mesh.devices.reshape(4, 4, mesh.shape["tp"]), ("z", "x", "tp"))
    placed = (
        P(SP, "tp"),
        P(SP, "tp"),
        P(SP, "tp"),
        P(SP, "tp"),
        P(SP, "tp"),
        P("tp", SP),
        P("tp", SP),
        P(SP),
        P("tp"),
        P("tp", None),
        P(),
        P(SP, "tp"),
        P(SP, "tp"),
        P(None, "tp"),
        P("tp", SP),
    )
    return jax.shard_map(body, mesh=torus, in_specs=placed, out_specs=P(SP, "tp"), check_vma=False)
```

```python
import jax
import jax.numpy as jnp
from jax import lax
from jax.experimental import pallas as pl
from jax.experimental.pallas import tpu as pltpu
from jax.sharding import Mesh
from jax.sharding import PartitionSpec as P


DH = 96
DOC_MAX = 3072
SP = ("z", "x")
TP = ("y", "c")
ABSENT = -1e30
HALO = 16
EPS = 1e-06
HEAD_FLOOR = 1.0
F32 = jnp.float32
BF16 = jnp.bfloat16


def in_first_head(shape):
    return lax.broadcasted_iota(jnp.int32, shape, len(shape) - 1) < DH


def state_kernel(k_ref, v_ref, in_ref, forget_ref, doc_ref, pay_ref, row_ref, col_ref, scr):
    tokens, width = k_ref.shape
    lane = lax.broadcasted_iota(jnp.int32, (8, tokens), 1)
    doc = jnp.broadcast_to(doc_ref[...].astype(F32), (8, tokens))
    scr[...] = jnp.zeros_like(scr)
    scr[0:2, :] = forget_ref[...]
    raw = scr[...]
    total = jnp.minimum(raw, 0.0) - jnp.log1p(jnp.exp(-jnp.abs(raw)))
    step = 1
    while step < tokens:
        total = total + jnp.where(lane >= step, pltpu.roll(total, step, 1), 0.0)
        step *= 2
    scr[0:2, :] = in_ref[...]
    rest = scr[...] - total
    peak = rest
    step = 1
    while step < tokens:
        near = (lane >= step) & (pltpu.roll(doc, step, 1) == doc)
        peak = jnp.maximum(peak, jnp.where(near, pltpu.roll(peak, step, 1), ABSENT))
        step *= 2
    end_doc = doc[:, tokens - 1 : tokens]
    end_peak = peak[:, tokens - 1 : tokens]
    end_total = total[:, tokens - 1 : tokens]
    weight = jnp.where(doc == end_doc, jnp.exp(jnp.minimum(rest - end_peak, 0.0)), 0.0)
    row_ref[...] = jnp.zeros_like(row_ref)
    row_ref[0:2, :] = total[0:2, :]
    row_ref[2:4, :] = peak[0:2, :]
    row_ref[4:6, :] = weight[0:2, :]
    row_ref[6:7, :] = doc[0:1, :]
    scr[...] = row_ref[...]
    cols = scr[...].T
    col_ref[...] = cols
    row_ref[4:6, :] = rest[0:2, :]
    first = in_first_head((tokens, width))
    spread = jnp.where(first, cols[:, 4:5], cols[:, 5:6])
    weighted = (k_ref[...].astype(F32) * (spread * DH**-0.5)).astype(BF16)
    state = lax.dot_general(
        weighted, v_ref[...], (((0,), (0,)), ((), ())), preferred_element_type=F32
    )
    small = in_first_head((DH, width))
    pay_ref[0:DH, :] = jnp.where(small, state[0:DH, :], state[DH:, :]).astype(BF16)

    line = in_first_head((1, width))

    def spread_heads(x):
        return jnp.where(line, x[0:1, :], x[1:2, :])

    def split(x):
        high = x.astype(BF16).astype(F32)
        mid = (x - high).astype(BF16).astype(F32)
        return high, mid, x - high - mid

    lines = [
        *split(spread_heads(end_total + end_peak)),
        *split(spread_heads(end_total)),
        jnp.broadcast_to(end_doc[0:1, :] + 1.0, (1, width)),
        jnp.broadcast_to(doc[0:1, tokens - 2 : tokens - 1] + 1.0, (1, width)),
    ]
    place = lax.broadcasted_iota(jnp.int32, (16, width), 0)
    table = jnp.zeros((16, width), F32)
    for k, value in enumerate(lines):
        table = jnp.where(place == k, value, table)
    pay_ref[DH:, :] = table.astype(BF16)


def local_kernel(q_ref, k_ref, v_ref, row_ref, col_ref, out_ref):
    tokens, width = q_ref.shape
    block = 256
    for start in range(0, tokens, block):
        stop = start + block
        keys = k_ref[0:stop, :]
        vals = v_ref[0:stop, :]
        q = q_ref[start:stop, :]
        first = in_first_head((block, width))
        at = lax.broadcasted_iota(jnp.int32, (block, stop), 0) + start
        source = lax.broadcasted_iota(jnp.int32, (block, stop), 1)
        seen = (at >= source) & (row_ref[6:7, 0:stop] == col_ref[start:stop, 6:7])
        found = []
        for h in range(2):
            mine = jnp.where(first if h == 0 else jnp.logical_not(first), q, jnp.zeros_like(q))
            scores = lax.dot_general(
                mine, keys, (((1,), (1,)), ((), ())), preferred_element_type=F32
            )
            gap = row_ref[4 + h : 5 + h, 0:stop] - col_ref[start:stop, 2 + h : 3 + h]
            part = (scores * jnp.exp(jnp.where(seen, gap, ABSENT))).astype(BF16)
            found.append(jnp.dot(part, vals, preferred_element_type=F32))
        out_ref[start:stop, :] = jnp.where(first, found[0], found[1])


def mix_kernel(
    order_ref, q_ref, gate_ref, local_ref, row_ref, col_ref, gain_ref, w_ref, *refs
):
    pays, (out_ref, near_ref, far_ref, mix_ref) = refs[:-4], refs[-4:]
    tokens, width = q_ref.shape

    @pl.when(pl.program_id(0) == 0)
    def _():
        own = row_ref[6:7, 0:1] + 1.0
        behind = jnp.zeros((1, width), F32)
        peaks, goods = [], []
        for ref in pays:
            table = ref[DH:, :].astype(F32)
            good = table[6:7, :] == own
            peaks.append(
                jnp.where(good, table[0:1, :] + table[1:2, :] + table[2:3, :] + behind, ABSENT)
            )
            goods.append(good)
            behind = behind + (table[3:4, :] + table[4:5, :] + table[5:6, :])
        best = peaks[0]
        for value in peaks[1:]:
            best = jnp.maximum(best, value)
        state = jnp.zeros((DH, width), F32)
        for ref, value, good in zip(pays, peaks, goods):
            state = state + jnp.where(good, jnp.exp(value - best), 0.0) * ref[0:DH, :].astype(F32)
        small = in_first_head((DH, width))
        whole = jnp.concatenate(
            [jnp.where(small, state, 0.0), jnp.where(small, 0.0, state)], axis=0
        ).astype(BF16)
        carried = jnp.dot(q_ref[...], whole, preferred_element_type=F32)
        first = in_first_head((tokens, width))
        total = jnp.where(first, col_ref[:, 0:1], col_ref[:, 1:2])
        peak = total + jnp.where(first, col_ref[:, 2:3], col_ref[:, 3:4])
        inter = jnp.where(col_ref[:, 6:7] + 1.0 == own, total + best, ABSENT)
        top = jnp.maximum(peak, inter)
        memory = (
            jnp.exp(peak - top) * (local_ref[...] * DH**-0.5) + jnp.exp(inter - top) * carried
        )
        square = memory * memory
        mean_0 = jnp.sum(jnp.where(first, square, 0.0), axis=1, keepdims=True) / DH
        mean_1 = jnp.sum(jnp.where(first, 0.0, square), axis=1, keepdims=True) / DH
        norm = jnp.where(first, lax.rsqrt(mean_0 + HEAD_FLOOR), lax.rsqrt(mean_1 + HEAD_FLOOR))
        gate = gate_ref[...].astype(F32)
        mix_ref[...] = (memory * norm * gain_ref[...] * (1.0 / (1.0 + jnp.exp(-gate)))).astype(BF16)

        ids = pays[0][DH:, :].astype(F32)
        last, second = ids[6:7, 0:1], ids[7:8, 0:1]
        doc = jnp.broadcast_to(col_ref[:, 6:7], (tokens, 128)) + 1.0
        row = lax.broadcasted_iota(jnp.int32, (tokens, 128), 0)
        one = jnp.where(row == 0, last, pltpu.roll(doc, 1, 0))
        two = jnp.where(row == 0, second, jnp.where(row == 1, last, pltpu.roll(doc, 2, 0)))
        near_ref[...] = (one == doc).astype(F32)
        far_ref[...] = (two == doc).astype(F32)

    out_ref[0] = jnp.dot(mix_ref[...], w_ref[...], preferred_element_type=F32).astype(BF16)


def norm_kernel(order_ref, *refs):
    pieces, (gain_ref, out_ref, send_ref) = refs[:-3], refs[-3:]
    tokens, cols = pieces[0].shape
    model = out_ref.shape[1]
    i = pl.program_id(0)
    square = jnp.zeros((tokens, cols), F32)
    for ref in pieces:
        r = ref[...].astype(F32)
        square = square + r * r
    mean = jnp.sum(square, axis=1, keepdims=True) / model
    scale = lax.rsqrt(mean + EPS)
    rows = pl.ds(pl.multiple_of(HALO + i * tokens, 16), tokens)
    for p, ref in enumerate(pieces):
        cut = pl.ds(pl.multiple_of(order_ref[p] * cols, 128), cols)
        done = (ref[...].astype(F32) * scale * gain_ref[0:1, cut]).astype(BF16)
        out_ref[rows, cut] = done
        send_ref[:, cut] = done[tokens - HALO :, :]


def mixer_kernel(
    order_ref,
    x_ref,
    near_ref,
    far_ref,
    taps_ref,
    wg_ref,
    wv_ref,
    wt_ref,
    wda_ref,
    wdb_ref,
    wdta_ref,
    wdtb_ref,
    out_ref,
    gate_scr,
    value_scr,
    h_scr,
):
    tokens = near_ref.shape[0]
    tiles, _, tile = taps_ref.shape
    tiles -= 1
    main = tiles * tile
    j = pl.program_id(0)

    def hidden(gate, value, taps, rows):
        near, far = near_ref[rows, :], far_ref[rows, :]
        one = pltpu.roll(gate, 1, 0)[HALO:, :]
        two = pltpu.roll(gate, 2, 0)[HALO:, :]
        conv = (
            taps[2:3, :] * gate[HALO:, :]
            + taps[1:2, :] * (near * one)
            + taps[0:1, :] * (far * two)
        )
        return conv / (1.0 + jnp.exp(-conv)) * value

    block = 96

    def finish(slot, at):
        for start in range(0, tokens, block):
            for half in range(0, tile, 128):
                lanes = slice(half, half + 128)
                done = hidden(
                    gate_scr[slot, start : start + block + HALO, lanes].astype(F32),
                    value_scr[slot, start + HALO : start + HALO + block, lanes].astype(F32),
                    taps_ref[at, :, lanes],
                    slice(start, start + block),
                )
                spot = pl.multiple_of(at * tile + half, 128)
                h_scr[start : start + block, pl.ds(spot, 128)] = done.astype(BF16)

    @pl.when(j < tiles)
    def _():
        gate_scr[j % 2] = jnp.dot(x_ref[...], wg_ref[...], preferred_element_type=F32).astype(BF16)
        value_scr[j % 2] = jnp.dot(x_ref[...], wv_ref[...], preferred_element_type=F32).astype(BF16)

    @pl.when((j > 0) & (j <= tiles))
    def _():
        finish((j - 1) % 2, j - 1)

    @pl.when(j == tiles)
    def _():
        both = jnp.dot(x_ref[...], wt_ref[...], preferred_element_type=F32).astype(BF16)
        for start in range(0, tokens, block):
            part = both[start : start + block + HALO, :].astype(F32)
            lane = lax.broadcasted_iota(jnp.int32, (block, 128), 1)
            mine = (lane >= 64) & (lane < 96)
            done = hidden(
                pltpu.roll(part, 64, 1),
                pltpu.roll(part, 32, 1)[HALO:, :],
                taps_ref[tiles, :, 0:128],
                slice(start, start + block),
            )
            h_scr[start : start + block, main:] = jnp.where(mine, done, 0.0).astype(BF16)

    @pl.when(j > tiles)
    def _():
        contract = (((1,), (1,)), ((), ()))
        for p, (wd_ref, wdt_ref) in enumerate(((wda_ref, wdta_ref), (wdb_ref, wdtb_ref))):
            out_ref[p] = (
                lax.dot_general(h_scr[:, 0:main], wd_ref[...], contract, preferred_element_type=F32)
                + lax.dot_general(
                    h_scr[:, main:], wdt_ref[...], contract, preferred_element_type=F32
                )
            ).astype(BF16)


def added(*terms):
    total = terms[0].astype(F32)
    for term in terms[1:]:
        total = total + term.astype(F32)
    return total


def shifted(value, by):
    ring = lax.axis_size("y")
    return lax.ppermute(value, "y", [(i, (i + by) % ring) for i in range(ring)])


def swapped(value):
    return lax.ppermute(value, "c", [(0, 1), (1, 0)])


def summed_over_tp(shares):
    half = shares.shape[2] // 2
    other = swapped(shares[1])
    pair = [added(shares[0, k], other[k]).astype(BF16) for k in range(4)]
    up = shifted(pair[2][:half], 1)
    down = shifted(pair[2][half:], -1)
    up = jnp.concatenate([added(pair[1][:half], up).astype(BF16), pair[1][half:]], axis=0)
    down = jnp.concatenate([pair[3][:half], added(pair[3][half:], down).astype(BF16)], axis=0)
    return added(pair[0], shifted(up, 1), shifted(down, -1))


def gathered_over_tp(own):
    half = own.shape[0] // 2
    below, above = shifted(own, 1), shifted(own, -1)
    far = jnp.concatenate([shifted(below[:half], 1), shifted(above[half:], -1)], axis=0)
    mine = [own, below, above, far]
    return mine + [swapped(part) for part in mine]


def shape(dims, dtype):
    return jax.ShapeDtypeStruct(dims, dtype)


def whole(dims):
    return pl.BlockSpec(dims, lambda *_: (0,) * len(dims))


def layer(
    resid,
    query,
    keys,
    values,
    out_gate,
    in_gate,
    forget,
    doc_ids,
    head_gain,
    w_out,
    ffn_gain,
    w_gate,
    w_value,
    conv_taps,
    w_down,
):
    tokens, width = query.shape
    cols = resid.shape[1]
    parts = w_out.shape[1] // cols
    model = w_out.shape[1]
    hidden = w_gate.shape[1]
    main = hidden // 128 * 128
    spare = hidden - main
    down_t = w_down.T
    packed = jnp.concatenate(
        [
            w_gate[:, :main],
            w_value[:, :main],
            down_t[:, :main],
            w_gate[:, main:],
            w_value[:, main:],
            down_t[:, main:],
            jnp.zeros((w_gate.shape[0], 128 - 3 * spare), BF16),
        ],
        axis=1,
    )
    weights = lax.all_gather(packed, SP, axis=0, tiled=True)
    tile = 256
    tiles = main // tile
    spot = 2 * spare
    taps = jnp.concatenate(
        [
            jnp.swapaxes(conv_taps[:, :main].reshape(3, tiles, tile), 0, 1),
            jnp.pad(conv_taps[:, main:], ((0, 0), (spot, tile - spot - spare)))[None],
        ],
        axis=0,
    )

    pay, rows, cols_aux = pl.pallas_call(
        state_kernel,
        out_shape=(
            shape((DH + 16, width), BF16),
            shape((8, tokens), F32),
            shape((tokens, 8), F32),
        ),
        scratch_shapes=[pltpu.VMEM((8, tokens), F32)],
        name="state",
    )(keys, values, in_gate, forget, doc_ids.reshape(1, tokens))
    count = lax.axis_size(SP)
    reach = -(-(DOC_MAX - 1) // tokens)
    pays = [
        lax.ppermute(pay, SP, [(i, i + k) for i in range(count - k)]) for k in range(1, reach + 1)
    ]
    local = pl.pallas_call(
        local_kernel,
        out_shape=shape((tokens, width), F32),
        name="local",
    )(query, keys, values, rows, cols_aux)
    chip, core = lax.axis_index("y"), lax.axis_index("c")
    ring, cores = lax.axis_size("y"), lax.axis_size("c")
    chips = (chip + jnp.arange(ring, dtype=jnp.int32)) % ring
    sides = core ^ jnp.arange(cores, dtype=jnp.int32)
    order = (chips[None, :] * cores + sides[:, None]).reshape(-1)
    share, near, far = pl.pallas_call(
        mix_kernel,
        grid_spec=pltpu.PrefetchScalarGridSpec(
            num_scalar_prefetch=1,
            grid=(parts,),
            in_specs=[
                whole((tokens, width)),
                whole((tokens, width)),
                whole((tokens, width)),
                whole((8, tokens)),
                whole((tokens, 8)),
                whole((1, width)),
                pl.BlockSpec((width, cols), lambda j, order: (0, order[j])),
                *[whole((DH + 16, width)) for _ in pays],
            ],
            out_specs=(
                pl.BlockSpec((1, tokens, cols), lambda j, order: (j, 0, 0)),
                whole((tokens, 128)),
                whole((tokens, 128)),
            ),
            scratch_shapes=[pltpu.VMEM((tokens, width), BF16)],
        ),
        out_shape=(
            shape((parts, tokens, cols), BF16),
            shape((tokens, 128), F32),
            shape((tokens, 128), F32),
        ),
        name="mix",
    )(order, query, out_gate, local, rows, cols_aux, head_gain.reshape(1, width), w_out, *pays)
    attended = summed_over_tp(share.reshape(cores, ring, tokens, cols))
    residual_own = resid.astype(F32) + attended
    pieces = gathered_over_tp(residual_own.astype(BF16))
    came = (chip + jnp.array([0, -1, 1, 2], jnp.int32)) % ring
    places = (came[None, :] * cores + sides[:, None]).reshape(-1)
    block = 96
    normed, send = pl.pallas_call(
        norm_kernel,
        grid_spec=pltpu.PrefetchScalarGridSpec(
            num_scalar_prefetch=1,
            grid=(tokens // block,),
            in_specs=[
                *[pl.BlockSpec((block, cols), lambda i, places: (i, 0)) for _ in pieces],
                whole((1, model)),
            ],
            out_specs=(whole((tokens + HALO, model)), whole((HALO, model))),
        ),
        out_shape=(shape((tokens + HALO, model), BF16), shape((HALO, model), BF16)),
        compiler_params=pltpu.CompilerParams(vmem_limit_bytes=40 * 2**20),
        name="norm",
    )(places, *pieces, ffn_gain.reshape(1, model))
    edge = lax.ppermute(send, SP, [(i, i + 1) for i in range(count - 1)])
    normed = lax.dynamic_update_slice(normed, edge, (0, 0))
    first = tiles + 1
    tail_at = 3 * main // 128

    def down_at(k, col):
        return lambda j, order: (order[2 * jnp.maximum(j - first, 0) + k], col)

    terms = pl.pallas_call(
        mixer_kernel,
        grid_spec=pltpu.PrefetchScalarGridSpec(
            num_scalar_prefetch=1,
            grid=(first + parts // 2,),
            in_specs=[
                pl.BlockSpec(
                    (tokens + HALO, model), lambda j, order: (0, 0), pipeline_mode=pl.Buffered(1)
                ),
                whole((tokens, 128)),
                whole((tokens, 128)),
                whole((tiles + 1, 3, tile)),
                pl.BlockSpec((model, tile), lambda j, order: (0, jnp.minimum(j, tiles - 1))),
                pl.BlockSpec(
                    (model, tile), lambda j, order: (0, tiles + jnp.minimum(j, tiles - 1))
                ),
                pl.BlockSpec((model, 128), lambda j, order: (0, tail_at)),
                pl.BlockSpec((cols, main), down_at(0, 2)),
                pl.BlockSpec((cols, main), down_at(1, 2)),
                pl.BlockSpec((cols, 128), down_at(0, tail_at)),
                pl.BlockSpec((cols, 128), down_at(1, tail_at)),
            ],
            out_specs=pl.BlockSpec(
                (2, tokens, cols), lambda j, order: (jnp.maximum(j - first, 0), 0, 0)
            ),
            scratch_shapes=[
                pltpu.VMEM((2, tokens + HALO, tile), BF16),
                pltpu.VMEM((2, tokens + HALO, tile), BF16),
                pltpu.VMEM((tokens, main + 128), BF16),
            ],
        ),
        out_shape=shape((parts, tokens, cols), BF16),
        compiler_params=pltpu.CompilerParams(vmem_limit_bytes=56 * 2**20),
        name="mixer",
    )(order, normed, near, far, taps, *[weights] * 7)
    down = summed_over_tp(terms.reshape(cores, ring, tokens, cols))
    return (residual_own + down).astype(BF16)


def solution(mesh):
    torus = Mesh(mesh.devices.reshape(4, 4, 4, 2), ("z", "x", "y", "c"))
    placed = (
        P(SP, TP),
        P(SP, TP),
        P(SP, TP),
        P(SP, TP),
        P(SP, TP),
        P(TP, SP),
        P(TP, SP),
        P(SP),
        P(TP),
        P(TP, None),
        P(),
        P(SP, TP),
        P(SP, TP),
        P(None, TP),
        P(TP, SP),
    )
    return jax.shard_map(layer, mesh=torus, in_specs=placed, out_specs=P(SP, TP), check_vma=False)
```

```python
import jax
import jax.numpy as jnp
from jax import lax
from jax.experimental import pallas as pl
from jax.experimental.pallas import tpu as pltpu
from jax.sharding import Mesh
from jax.sharding import PartitionSpec as P


DH = 96
DOC_MAX = 3072
SP = ("z", "x")
TP = ("y", "c")
ABSENT = -1e30
HALO = 16
EPS = 1e-06
HEAD_FLOOR = 1.0
F32 = jnp.float32
BF16 = jnp.bfloat16


def in_first_head(shape):
    return lax.broadcasted_iota(jnp.int32, shape, len(shape) - 1) < DH


def pack_kernel(gate_ref, value_ref, down_ref, out_ref):
    rows, hidden = gate_ref.shape
    main = hidden // 128 * 128
    tails = []
    for k, ref in enumerate((gate_ref, value_ref, down_ref)):
        out_ref[:, k * main : (k + 1) * main] = ref[:, :main]
        tails.append(ref[:, main:])
    tails.append(jnp.zeros((rows, 128 - 3 * (hidden - main)), BF16))
    out_ref[:, 3 * main :] = jnp.concatenate(tails, axis=1)


def state_kernel(k_ref, v_ref, in_ref, forget_ref, doc_ref, pay_ref, row_ref, col_ref, scr):
    tokens, width = k_ref.shape
    lane = lax.broadcasted_iota(jnp.int32, (8, tokens), 1)
    doc = jnp.broadcast_to(doc_ref[...].astype(F32), (8, tokens))
    scr[...] = jnp.zeros_like(scr)
    scr[0:2, :] = forget_ref[...]
    raw = scr[...]
    total = jnp.minimum(raw, 0.0) - jnp.log1p(jnp.exp(-jnp.abs(raw)))
    step = 1
    while step < tokens:
        total = total + jnp.where(lane >= step, pltpu.roll(total, step, 1), 0.0)
        step *= 2
    scr[0:2, :] = in_ref[...]
    rest = scr[...] - total
    peak = rest
    step = 1
    while step < tokens:
        near = (lane >= step) & (pltpu.roll(doc, step, 1) == doc)
        peak = jnp.maximum(peak, jnp.where(near, pltpu.roll(peak, step, 1), ABSENT))
        step *= 2
    end_doc = doc[:, tokens - 1 : tokens]
    end_peak = peak[:, tokens - 1 : tokens]
    end_total = total[:, tokens - 1 : tokens]
    weight = jnp.where(doc == end_doc, jnp.exp(jnp.minimum(rest - end_peak, 0.0)), 0.0)
    row_ref[...] = jnp.zeros_like(row_ref)
    row_ref[0:2, :] = total[0:2, :]
    row_ref[2:4, :] = peak[0:2, :]
    row_ref[4:6, :] = weight[0:2, :]
    row_ref[6:7, :] = doc[0:1, :]
    scr[...] = row_ref[...]
    cols = scr[...].T
    col_ref[...] = cols
    row_ref[4:6, :] = rest[0:2, :]
    first = in_first_head((tokens, width))
    spread = jnp.where(first, cols[:, 4:5], cols[:, 5:6])
    weighted = (k_ref[...].astype(F32) * (spread * DH**-0.5)).astype(BF16)
    state = lax.dot_general(
        weighted, v_ref[...], (((0,), (0,)), ((), ())), preferred_element_type=F32
    )
    small = in_first_head((DH, width))
    pay_ref[0:DH, :] = jnp.where(small, state[0:DH, :], state[DH:, :]).astype(BF16)

    line = in_first_head((1, width))

    def spread_heads(x):
        return jnp.where(line, x[0:1, :], x[1:2, :])

    def split(x):
        high = x.astype(BF16).astype(F32)
        mid = (x - high).astype(BF16).astype(F32)
        return high, mid, x - high - mid

    lines = [
        *split(spread_heads(end_total + end_peak)),
        *split(spread_heads(end_total)),
        jnp.broadcast_to(end_doc[0:1, :] + 1.0, (1, width)),
        jnp.broadcast_to(doc[0:1, tokens - 2 : tokens - 1] + 1.0, (1, width)),
    ]
    place = lax.broadcasted_iota(jnp.int32, (16, width), 0)
    table = jnp.zeros((16, width), F32)
    for k, value in enumerate(lines):
        table = jnp.where(place == k, value, table)
    pay_ref[DH:, :] = table.astype(BF16)


def local_kernel(q_ref, k_ref, v_ref, row_ref, col_ref, out_ref):
    tokens, width = q_ref.shape
    block = 256
    for start in range(0, tokens, block):
        stop = start + block
        keys = k_ref[0:stop, :]
        vals = v_ref[0:stop, :]
        q = q_ref[start:stop, :]
        first = in_first_head((block, width))
        at = lax.broadcasted_iota(jnp.int32, (block, stop), 0) + start
        source = lax.broadcasted_iota(jnp.int32, (block, stop), 1)
        seen = (at >= source) & (row_ref[6:7, 0:stop] == col_ref[start:stop, 6:7])
        found = []
        for h in range(2):
            mine = jnp.where(first if h == 0 else jnp.logical_not(first), q, jnp.zeros_like(q))
            scores = lax.dot_general(
                mine, keys, (((1,), (1,)), ((), ())), preferred_element_type=F32
            )
            gap = row_ref[4 + h : 5 + h, 0:stop] - col_ref[start:stop, 2 + h : 3 + h]
            part = (scores * jnp.exp(jnp.where(seen, gap, ABSENT))).astype(BF16)
            found.append(jnp.dot(part, vals, preferred_element_type=F32))
        out_ref[start:stop, :] = jnp.where(first, found[0], found[1])


def mix_kernel(
    order_ref, q_ref, gate_ref, local_ref, row_ref, col_ref, gain_ref, w_ref, *refs
):
    pays, (out_ref, near_ref, far_ref, mix_ref) = refs[:-4], refs[-4:]
    tokens, width = q_ref.shape

    @pl.when(pl.program_id(0) == 0)
    def _():
        own = row_ref[6:7, 0:1] + 1.0
        behind = jnp.zeros((1, width), F32)
        peaks, goods = [], []
        for ref in pays:
            table = ref[DH:, :].astype(F32)
            good = table[6:7, :] == own
            peaks.append(
                jnp.where(good, table[0:1, :] + table[1:2, :] + table[2:3, :] + behind, ABSENT)
            )
            goods.append(good)
            behind = behind + (table[3:4, :] + table[4:5, :] + table[5:6, :])
        best = peaks[0]
        for value in peaks[1:]:
            best = jnp.maximum(best, value)
        state = jnp.zeros((DH, width), F32)
        for ref, value, good in zip(pays, peaks, goods):
            state = state + jnp.where(good, jnp.exp(value - best), 0.0) * ref[0:DH, :].astype(F32)
        small = in_first_head((DH, width))
        whole = jnp.concatenate(
            [jnp.where(small, state, 0.0), jnp.where(small, 0.0, state)], axis=0
        ).astype(BF16)
        carried = jnp.dot(q_ref[...], whole, preferred_element_type=F32)
        first = in_first_head((tokens, width))
        total = jnp.where(first, col_ref[:, 0:1], col_ref[:, 1:2])
        peak = total + jnp.where(first, col_ref[:, 2:3], col_ref[:, 3:4])
        inter = jnp.where(col_ref[:, 6:7] + 1.0 == own, total + best, ABSENT)
        top = jnp.maximum(peak, inter)
        memory = (
            jnp.exp(peak - top) * (local_ref[...] * DH**-0.5) + jnp.exp(inter - top) * carried
        )
        square = memory * memory
        mean_0 = jnp.sum(jnp.where(first, square, 0.0), axis=1, keepdims=True) / DH
        mean_1 = jnp.sum(jnp.where(first, 0.0, square), axis=1, keepdims=True) / DH
        norm = jnp.where(first, lax.rsqrt(mean_0 + HEAD_FLOOR), lax.rsqrt(mean_1 + HEAD_FLOOR))
        gate = gate_ref[...].astype(F32)
        mix_ref[...] = (memory * norm * gain_ref[...] * (1.0 / (1.0 + jnp.exp(-gate)))).astype(BF16)

        ids = pays[0][DH:, :].astype(F32)
        last, second = ids[6:7, 0:1], ids[7:8, 0:1]
        doc = jnp.broadcast_to(col_ref[:, 6:7], (tokens, 128)) + 1.0
        row = lax.broadcasted_iota(jnp.int32, (tokens, 128), 0)
        one = jnp.where(row == 0, last, pltpu.roll(doc, 1, 0))
        two = jnp.where(row == 0, second, jnp.where(row == 1, last, pltpu.roll(doc, 2, 0)))
        near_ref[...] = (one == doc).astype(F32)
        far_ref[...] = (two == doc).astype(F32)

    out_ref[0] = jnp.dot(mix_ref[...], w_ref[...], preferred_element_type=F32).astype(BF16)


def norm_kernel(order_ref, *refs):
    pieces, (gain_ref, out_ref, send_ref) = refs[:-3], refs[-3:]
    tokens, cols = pieces[0].shape
    model = out_ref.shape[1]
    i = pl.program_id(0)
    square = jnp.zeros((tokens, cols), F32)
    for ref in pieces:
        r = ref[...].astype(F32)
        square = square + r * r
    mean = jnp.sum(square, axis=1, keepdims=True) / model
    scale = lax.rsqrt(mean + EPS)
    rows = pl.ds(pl.multiple_of(HALO + i * tokens, 16), tokens)
    for p, ref in enumerate(pieces):
        cut = pl.ds(pl.multiple_of(order_ref[p] * cols, 128), cols)
        done = (ref[...].astype(F32) * scale * gain_ref[0:1, cut]).astype(BF16)
        out_ref[rows, cut] = done
        send_ref[:, cut] = done[tokens - HALO :, :]


def down_product(h, w):
    return lax.dot_general(
        h, w, (((1,), (1,)), ((), ())), preferred_element_type=F32
    ).astype(BF16)


def mixer_kernel(
    order_ref,
    x_ref,
    near_ref,
    far_ref,
    taps_ref,
    wg_ref,
    wv_ref,
    w_ref,
    h_ref,
    swap_ref,
    own_ref,
    gate_scr,
    value_scr,
    tail_scr,
    down_scr,
    sems,
):
    tokens = near_ref.shape[0]
    tiles, _, tile = taps_ref.shape
    tiles -= 1
    main = tiles * tile
    cols = down_scr.shape[1]
    j = pl.program_id(0)
    copies = [pltpu.make_async_copy(w_ref.at[:, pl.ds(3 * main, 128)], tail_scr, sems.at[0])]
    for k in range(2):
        rows = pl.ds(pl.multiple_of(order_ref[k] * cols, 128), cols)
        copies.append(
            pltpu.make_async_copy(
                w_ref.at[rows, pl.ds(2 * main, main)],
                down_scr.at[k, :, pl.ds(0, main)],
                sems.at[1 + 2 * k],
            )
        )
        copies.append(
            pltpu.make_async_copy(
                w_ref.at[rows, pl.ds(3 * main, 128)],
                down_scr.at[k, :, pl.ds(main, 128)],
                sems.at[2 + 2 * k],
            )
        )

    def hidden(gate, value, taps, rows):
        near, far = near_ref[rows, :], far_ref[rows, :]
        one = pltpu.roll(gate, 1, 0)[HALO:, :]
        two = pltpu.roll(gate, 2, 0)[HALO:, :]
        conv = (
            taps[2:3, :] * gate[HALO:, :]
            + taps[1:2, :] * (near * one)
            + taps[0:1, :] * (far * two)
        )
        scaled = 0.5 * conv
        return (scaled + scaled * jnp.tanh(scaled)) * value

    block = 96

    def finish(slot, at):
        for start in range(0, tokens, block):
            for half in range(0, tile, 128):
                lanes = slice(half, half + 128)
                done = hidden(
                    gate_scr[slot, start : start + block + HALO, lanes],
                    value_scr[slot, start + HALO : start + HALO + block, lanes],
                    taps_ref[at, :, lanes],
                    slice(start, start + block),
                )
                spot = pl.multiple_of(at * tile + half, 128)
                h_ref[start : start + block, pl.ds(spot, 128)] = done.astype(BF16)

    def project(slot):
        gate_scr[slot] = jnp.dot(x_ref[...], wg_ref[...], preferred_element_type=F32)
        value_scr[slot] = jnp.dot(x_ref[...], wv_ref[...], preferred_element_type=F32)

    @pl.when(j == 0)
    def _():
        for copy in copies:
            copy.start()
        project(0)

    @pl.when((j > 0) & (j < tiles))
    def _():
        project(j % 2)
        finish((j - 1) % 2, j - 1)

    @pl.when(j == tiles)
    def _():
        copies[0].wait()
        both = jnp.dot(x_ref[...], tail_scr[...], preferred_element_type=F32)
        finish((tiles - 1) % 2, tiles - 1)
        for start in range(0, tokens, block):
            part = both[start : start + block + HALO, :]
            lane = lax.broadcasted_iota(jnp.int32, (block, 128), 1)
            mine = (lane >= 64) & (lane < 96)
            done = hidden(
                pltpu.roll(part, 64, 1),
                pltpu.roll(part, 32, 1)[HALO:, :],
                taps_ref[tiles, :, 0:128],
                slice(start, start + block),
            )
            h_ref[start : start + block, main:] = jnp.where(mine, done, 0.0).astype(BF16)

    @pl.when(j > tiles)
    def _():
        for copy in copies[1:]:
            copy.wait()
        swap_ref[0] = down_product(h_ref[...], down_scr[0])
        own_ref[0] = down_product(h_ref[...], down_scr[1])


def down_kernel(order_ref, h_ref, wa_ref, wb_ref, ta_ref, tb_ref, swap_ref, own_ref):
    count = swap_ref.shape[0]
    main = wa_ref.shape[1]
    both = ((wa_ref, ta_ref), (wb_ref, tb_ref))

    def put(ref, k, w_ref, t_ref):
        ref[k] = (
            lax.dot_general(
                h_ref[:, :main], w_ref[...], (((1,), (1,)), ((), ())), preferred_element_type=F32
            )
            + lax.dot_general(
                h_ref[:, main:], t_ref[...], (((1,), (1,)), ((), ())), preferred_element_type=F32
            )
        ).astype(BF16)

    if count == 1:
        put(swap_ref, 0, *both[0])
        put(own_ref, 0, *both[1])
        return

    @pl.when(pl.program_id(0) == 0)
    def _():
        for k in range(2):
            put(swap_ref, k, *both[k])

    @pl.when(pl.program_id(0) == 1)
    def _():
        for k in range(2):
            put(own_ref, k, *both[k])


def added(*terms):
    total = terms[0].astype(F32)
    for term in terms[1:]:
        total = total + term.astype(F32)
    return total


def shifted(value, by):
    ring = lax.axis_size("y")
    return lax.ppermute(value, "y", [(i, (i + by) % ring) for i in range(ring)])


def swapped(value):
    return lax.ppermute(value, "c", [(0, 1), (1, 0)])


def summed_over_tp(far, sides, near):
    swap, own = far()
    pair = added(own[0], swapped(swap)[0]).astype(BF16)
    half = pair.shape[0] // 2
    up = shifted(pair[:half], 1)
    down = shifted(pair[half:], -1)
    swap, own = sides()
    other = swapped(swap)
    pair = [added(own[k], other[k]) for k in range(2)]
    up = jnp.concatenate([added(pair[0][:half], up), pair[0][half:]], axis=0).astype(BF16)
    down = jnp.concatenate([pair[1][:half], added(pair[1][half:], down)], axis=0).astype(BF16)
    up = shifted(up, 1)
    down = shifted(down, -1)
    swap, own = near()
    return added(own[0], swapped(swap)[0], up, down)


def gathered_over_tp(own):
    half = own.shape[0] // 2
    below, above = shifted(own, 1), shifted(own, -1)
    far = jnp.concatenate([shifted(below[:half], 1), shifted(above[half:], -1)], axis=0)
    mine = [own, below, above, far]
    return mine + [swapped(part) for part in mine]


def shape(dims, dtype):
    return jax.ShapeDtypeStruct(dims, dtype)


def whole(dims):
    return pl.BlockSpec(dims, lambda *_: (0,) * len(dims))


def layer(
    resid,
    query,
    keys,
    values,
    out_gate,
    in_gate,
    forget,
    doc_ids,
    head_gain,
    w_out,
    ffn_gain,
    w_gate,
    w_value,
    conv_taps,
    w_down,
):
    tokens, width = query.shape
    cols = resid.shape[1]
    parts = w_out.shape[1] // cols
    model = w_out.shape[1]
    hidden = w_gate.shape[1]
    main = hidden // 128 * 128
    spare = hidden - main
    packed = pl.pallas_call(
        pack_kernel,
        out_shape=shape((w_gate.shape[0], 3 * main + 128), BF16),
        name="pack",
    )(w_gate, w_value, w_down.T)
    weights = lax.all_gather(packed, SP, axis=0, tiled=True)
    tile = 256
    tiles = main // tile
    spot = 2 * spare
    taps = jnp.concatenate(
        [
            jnp.swapaxes(conv_taps[:, :main].reshape(3, tiles, tile), 0, 1),
            jnp.pad(conv_taps[:, main:], ((0, 0), (spot, tile - spot - spare)))[None],
        ],
        axis=0,
    )

    pay, rows, cols_aux = pl.pallas_call(
        state_kernel,
        out_shape=(
            shape((DH + 16, width), BF16),
            shape((8, tokens), F32),
            shape((tokens, 8), F32),
        ),
        scratch_shapes=[pltpu.VMEM((8, tokens), F32)],
        name="state",
    )(keys, values, in_gate, forget, doc_ids.reshape(1, tokens))
    count = lax.axis_size(SP)
    reach = -(-(DOC_MAX - 1) // tokens)
    pays = [
        lax.ppermute(pay, SP, [(i, i + k) for i in range(count - k)]) for k in range(1, reach + 1)
    ]
    local = pl.pallas_call(
        local_kernel,
        out_shape=shape((tokens, width), F32),
        name="local",
    )(query, keys, values, rows, cols_aux)
    chip, core = lax.axis_index("y"), lax.axis_index("c")
    ring, cores = lax.axis_size("y"), lax.axis_size("c")
    chips = (chip + jnp.arange(ring, dtype=jnp.int32)) % ring
    sides = core ^ jnp.arange(cores, dtype=jnp.int32)
    to = chips[None, :] * cores + sides[:, None]
    order = jnp.stack([to[1, 2], to[0, 2], to[1, 1], to[1, 3], to[0, 1], to[0, 3], to[1, 0], to[0, 0]])
    share, near, far_flags = pl.pallas_call(
        mix_kernel,
        grid_spec=pltpu.PrefetchScalarGridSpec(
            num_scalar_prefetch=1,
            grid=(parts,),
            in_specs=[
                whole((tokens, width)),
                whole((tokens, width)),
                whole((tokens, width)),
                whole((8, tokens)),
                whole((tokens, 8)),
                whole((1, width)),
                pl.BlockSpec((width, cols), lambda j, order: (0, order[j])),
                *[whole((DH + 16, width)) for _ in pays],
            ],
            out_specs=(
                pl.BlockSpec((1, tokens, cols), lambda j, order: (j, 0, 0)),
                whole((tokens, 128)),
                whole((tokens, 128)),
            ),
            scratch_shapes=[pltpu.VMEM((tokens, width), BF16)],
        ),
        out_shape=(
            shape((parts, tokens, cols), BF16),
            shape((tokens, 128), F32),
            shape((tokens, 128), F32),
        ),
        name="mix",
    )(order, query, out_gate, local, rows, cols_aux, head_gain.reshape(1, width), w_out, *pays)
    attended = summed_over_tp(
        lambda: (share[0:1], share[1:2]),
        lambda: (share[2:4], share[4:6]),
        lambda: (share[6:7], share[7:8]),
    )
    residual_own = resid.astype(F32) + attended
    pieces = gathered_over_tp(residual_own.astype(BF16))
    came = (chip + jnp.array([0, -1, 1, 2], jnp.int32)) % ring
    places = (came[None, :] * cores + sides[:, None]).reshape(-1)
    block = 96
    normed, send = pl.pallas_call(
        norm_kernel,
        grid_spec=pltpu.PrefetchScalarGridSpec(
            num_scalar_prefetch=1,
            grid=(tokens // block,),
            in_specs=[
                *[pl.BlockSpec((block, cols), lambda i, places: (i, 0)) for _ in pieces],
                whole((1, model)),
            ],
            out_specs=(whole((tokens + HALO, model)), whole((HALO, model))),
        ),
        out_shape=(shape((tokens + HALO, model), BF16), shape((HALO, model), BF16)),
        compiler_params=pltpu.CompilerParams(vmem_limit_bytes=40 * 2**20),
        name="norm",
    )(places, *pieces, ffn_gain.reshape(1, model))
    edge = lax.ppermute(send, SP, [(i, i + 1) for i in range(count - 1)])
    normed = lax.dynamic_update_slice(normed, edge, (0, 0))
    tail_at = 3 * main // 128
    part = shape((1, tokens, cols), BF16)

    def far():
        return pl.pallas_call(
            mixer_kernel,
            grid_spec=pltpu.PrefetchScalarGridSpec(
                num_scalar_prefetch=1,
                grid=(tiles + 2,),
                in_specs=[
                    pl.BlockSpec(
                        (tokens + HALO, model),
                        lambda j, order: (0, 0),
                        pipeline_mode=pl.Buffered(1),
                    ),
                    whole((tokens, 128)),
                    whole((tokens, 128)),
                    whole((tiles + 1, 3, tile)),
                    pl.BlockSpec((model, tile), lambda j, order: (0, jnp.minimum(j, tiles - 1))),
                    pl.BlockSpec(
                        (model, tile), lambda j, order: (0, tiles + jnp.minimum(j, tiles - 1))
                    ),
                    pl.BlockSpec(memory_space=pl.ANY),
                ],
                out_specs=(
                    whole((tokens, main + 128)),
                    whole((1, tokens, cols)),
                    whole((1, tokens, cols)),
                ),
                scratch_shapes=[
                    pltpu.VMEM((2, tokens + HALO, tile), F32),
                    pltpu.VMEM((2, tokens + HALO, tile), F32),
                    pltpu.VMEM((model, 128), BF16),
                    pltpu.VMEM((2, cols, main + 128), BF16),
                    pltpu.SemaphoreType.DMA((5,)),
                ],
            ),
            out_shape=(shape((tokens, main + 128), BF16), part, part),
            compiler_params=pltpu.CompilerParams(vmem_limit_bytes=56 * 2**20),
            name="mixer",
        )(order, normed, near, far_flags, taps, weights, weights, weights)

    hidden, *far_parts = far()

    def further(at, count):
        def spot(k, col):
            return lambda j, order: (order[at + 2 * j + k], col)

        many = shape((count, tokens, cols), BF16)
        return pl.pallas_call(
            down_kernel,
            grid_spec=pltpu.PrefetchScalarGridSpec(
                num_scalar_prefetch=1,
                grid=(count,),
                in_specs=[
                    whole((tokens, main + 128)),
                    pl.BlockSpec((cols, main), spot(0, 2)),
                    pl.BlockSpec((cols, main), spot(1, 2)),
                    pl.BlockSpec((cols, 128), spot(0, tail_at)),
                    pl.BlockSpec((cols, 128), spot(1, tail_at)),
                ],
                out_specs=(whole((count, tokens, cols)), whole((count, tokens, cols))),
            ),
            out_shape=(many, many),
            compiler_params=pltpu.CompilerParams(vmem_limit_bytes=40 * 2**20),
        )(order, hidden, *[weights] * 4)

    down = summed_over_tp(lambda: far_parts, lambda: further(2, 2), lambda: further(6, 1))
    return (residual_own + down).astype(BF16)


def solution(mesh):
    torus = Mesh(mesh.devices.reshape(4, 4, 4, 2), ("z", "x", "y", "c"))
    placed = (
        P(SP, TP),
        P(SP, TP),
        P(SP, TP),
        P(SP, TP),
        P(SP, TP),
        P(TP, SP),
        P(TP, SP),
        P(SP),
        P(TP),
        P(TP, None),
        P(),
        P(SP, TP),
        P(SP, TP),
        P(None, TP),
        P(TP, SP),
    )
    return jax.shard_map(layer, mesh=torus, in_specs=placed, out_specs=P(SP, TP), check_vma=False)
```

```python
import jax
import jax.numpy as jnp
from jax import lax
from jax.experimental import pallas as pl
from jax.experimental.pallas import tpu as pltpu
from jax.sharding import Mesh
from jax.sharding import PartitionSpec as P


DH = 96
DOC_MAX = 3072
SP = ("z", "x")
TP = ("y", "c")
ABSENT = -1e30
HALO = 16
EPS = 1e-06
HEAD_FLOOR = 1.0
F32 = jnp.float32
BF16 = jnp.bfloat16


def in_first_head(shape):
    return lax.broadcasted_iota(jnp.int32, shape, len(shape) - 1) < DH


def pack_kernel(gate_ref, value_ref, down_ref, out_ref):
    rows, hidden = gate_ref.shape
    main = hidden // 128 * 128
    tails = []
    for k, ref in enumerate((gate_ref, value_ref, down_ref)):
        out_ref[:, k * main : (k + 1) * main] = ref[:, :main]
        tails.append(ref[:, main:])
    tails.append(jnp.zeros((rows, 128 - 3 * (hidden - main)), BF16))
    out_ref[:, 3 * main :] = jnp.concatenate(tails, axis=1)


def state_kernel(k_ref, v_ref, in_ref, forget_ref, doc_ref, pay_ref, row_ref, col_ref, scr):
    tokens, width = k_ref.shape
    lane = lax.broadcasted_iota(jnp.int32, (8, tokens), 1)
    doc = jnp.broadcast_to(doc_ref[...].astype(F32), (8, tokens))
    scr[...] = jnp.zeros_like(scr)
    scr[0:2, :] = forget_ref[...]
    raw = scr[...]
    total = jnp.minimum(raw, 0.0) - jnp.log1p(jnp.exp(-jnp.abs(raw)))
    step = 1
    while step < tokens:
        total = total + jnp.where(lane >= step, pltpu.roll(total, step, 1), 0.0)
        step *= 2
    scr[0:2, :] = in_ref[...]
    rest = scr[...] - total
    peak = rest
    step = 1
    while step < tokens:
        near = (lane >= step) & (pltpu.roll(doc, step, 1) == doc)
        peak = jnp.maximum(peak, jnp.where(near, pltpu.roll(peak, step, 1), ABSENT))
        step *= 2
    end_doc = doc[:, tokens - 1 : tokens]
    end_peak = peak[:, tokens - 1 : tokens]
    end_total = total[:, tokens - 1 : tokens]
    weight = jnp.where(doc == end_doc, jnp.exp(jnp.minimum(rest - end_peak, 0.0)), 0.0)
    row_ref[...] = jnp.zeros_like(row_ref)
    row_ref[0:2, :] = total[0:2, :]
    row_ref[2:4, :] = peak[0:2, :]
    row_ref[4:6, :] = weight[0:2, :]
    row_ref[6:7, :] = doc[0:1, :]
    scr[...] = row_ref[...]
    cols = scr[...].T
    col_ref[...] = cols
    row_ref[4:6, :] = rest[0:2, :]
    first = in_first_head((tokens, width))
    spread = jnp.where(first, cols[:, 4:5], cols[:, 5:6])
    weighted = (k_ref[...].astype(F32) * (spread * DH**-0.5)).astype(BF16)
    state = lax.dot_general(
        weighted, v_ref[...], (((0,), (0,)), ((), ())), preferred_element_type=F32
    )
    small = in_first_head((DH, width))
    pay_ref[0:DH, :] = jnp.where(small, state[0:DH, :], state[DH:, :]).astype(BF16)

    line = in_first_head((1, width))

    def spread_heads(x):
        return jnp.where(line, x[0:1, :], x[1:2, :])

    def split(x):
        high = x.astype(BF16).astype(F32)
        mid = (x - high).astype(BF16).astype(F32)
        return high, mid, x - high - mid

    lines = [
        *split(spread_heads(end_total + end_peak)),
        *split(spread_heads(end_total)),
        jnp.broadcast_to(end_doc[0:1, :] + 1.0, (1, width)),
        jnp.broadcast_to(doc[0:1, tokens - 2 : tokens - 1] + 1.0, (1, width)),
    ]
    place = lax.broadcasted_iota(jnp.int32, (16, width), 0)
    table = jnp.zeros((16, width), F32)
    for k, value in enumerate(lines):
        table = jnp.where(place == k, value, table)
    pay_ref[DH:, :] = table.astype(BF16)


def local_kernel(q_ref, k_ref, v_ref, row_ref, col_ref, out_ref):
    tokens, width = q_ref.shape
    block = 256
    for start in range(0, tokens, block):
        stop = start + block
        keys = k_ref[0:stop, :]
        vals = v_ref[0:stop, :]
        q = q_ref[start:stop, :]
        first = in_first_head((block, width))
        at = lax.broadcasted_iota(jnp.int32, (block, stop), 0) + start
        source = lax.broadcasted_iota(jnp.int32, (block, stop), 1)
        seen = (at >= source) & (row_ref[6:7, 0:stop] == col_ref[start:stop, 6:7])
        found = []
        for h in range(2):
            mine = jnp.where(first if h == 0 else jnp.logical_not(first), q, jnp.zeros_like(q))
            scores = lax.dot_general(
                mine, keys, (((1,), (1,)), ((), ())), preferred_element_type=F32
            )
            gap = row_ref[4 + h : 5 + h, 0:stop] - col_ref[start:stop, 2 + h : 3 + h]
            part = (scores * jnp.exp(jnp.where(seen, gap, ABSENT))).astype(BF16)
            found.append(jnp.dot(part, vals, preferred_element_type=F32))
        out_ref[start:stop, :] = jnp.where(first, found[0], found[1])


def mix_kernel(
    order_ref, q_ref, gate_ref, local_ref, row_ref, col_ref, gain_ref, w_ref, *refs
):
    w_own_ref, *pays = refs[:-5]
    swap_ref, own_out_ref, near_ref, far_ref, mix_ref = refs[-5:]
    tokens, width = q_ref.shape

    @pl.when(pl.program_id(0) == 0)
    def _():
        own = row_ref[6:7, 0:1] + 1.0
        behind = jnp.zeros((1, width), F32)
        peaks, goods = [], []
        for ref in pays:
            table = ref[DH:, :].astype(F32)
            good = table[6:7, :] == own
            peaks.append(
                jnp.where(good, table[0:1, :] + table[1:2, :] + table[2:3, :] + behind, ABSENT)
            )
            goods.append(good)
            behind = behind + (table[3:4, :] + table[4:5, :] + table[5:6, :])
        best = peaks[0]
        for value in peaks[1:]:
            best = jnp.maximum(best, value)
        state = jnp.zeros((DH, width), F32)
        for ref, value, good in zip(pays, peaks, goods):
            state = state + jnp.where(good, jnp.exp(value - best), 0.0) * ref[0:DH, :].astype(F32)
        small = in_first_head((DH, width))
        whole = jnp.concatenate(
            [jnp.where(small, state, 0.0), jnp.where(small, 0.0, state)], axis=0
        ).astype(BF16)
        carried = jnp.dot(q_ref[...], whole, preferred_element_type=F32)
        first = in_first_head((tokens, width))
        total = jnp.where(first, col_ref[:, 0:1], col_ref[:, 1:2])
        peak = total + jnp.where(first, col_ref[:, 2:3], col_ref[:, 3:4])
        inter = jnp.where(col_ref[:, 6:7] + 1.0 == own, total + best, ABSENT)
        top = jnp.maximum(peak, inter)
        memory = (
            jnp.exp(peak - top) * (local_ref[...] * DH**-0.5) + jnp.exp(inter - top) * carried
        )
        square = memory * memory
        mean_0 = jnp.sum(jnp.where(first, square, 0.0), axis=1, keepdims=True) / DH
        mean_1 = jnp.sum(jnp.where(first, 0.0, square), axis=1, keepdims=True) / DH
        norm = jnp.where(first, lax.rsqrt(mean_0 + HEAD_FLOOR), lax.rsqrt(mean_1 + HEAD_FLOOR))
        gate = gate_ref[...].astype(F32)
        mix_ref[...] = (memory * norm * gain_ref[...] * (1.0 / (1.0 + jnp.exp(-gate)))).astype(BF16)

        ids = pays[0][DH:, :].astype(F32)
        last, second = ids[6:7, 0:1], ids[7:8, 0:1]
        doc = jnp.broadcast_to(col_ref[:, 6:7], (tokens, 128)) + 1.0
        row = lax.broadcasted_iota(jnp.int32, (tokens, 128), 0)
        one = jnp.where(row == 0, last, pltpu.roll(doc, 1, 0))
        two = jnp.where(row == 0, second, jnp.where(row == 1, last, pltpu.roll(doc, 2, 0)))
        near_ref[...] = (one == doc).astype(F32)
        far_ref[...] = (two == doc).astype(F32)

    mix = mix_ref[...]
    swap_ref[0] = jnp.dot(mix, w_ref[...], preferred_element_type=F32).astype(BF16)
    own_out_ref[0] = jnp.dot(mix, w_own_ref[...], preferred_element_type=F32).astype(BF16)


def norm_kernel(order_ref, *refs):
    pieces, (gain_ref, out_ref, send_ref) = refs[:-3], refs[-3:]
    tokens, cols = pieces[0].shape
    model = out_ref.shape[1]
    i = pl.program_id(0)
    square = jnp.zeros((tokens, cols), F32)
    for ref in pieces:
        r = ref[...].astype(F32)
        square = square + r * r
    mean = jnp.sum(square, axis=1, keepdims=True) / model
    scale = lax.rsqrt(mean + EPS)
    rows = pl.ds(pl.multiple_of(HALO + i * tokens, 16), tokens)
    for p, ref in enumerate(pieces):
        cut = pl.ds(pl.multiple_of(order_ref[p] * cols, 128), cols)
        done = (ref[...].astype(F32) * scale * gain_ref[0:1, cut]).astype(BF16)
        out_ref[rows, cut] = done
        send_ref[:, cut] = done[tokens - HALO :, :]


def mixer_kernel(
    order_ref,
    x_ref,
    near_ref,
    far_ref,
    taps_ref,
    wg_ref,
    wv_ref,
    wt_ref,
    w_ref,
    h_ref,
    swap_ref,
    own_ref,
    gate_scr,
    value_scr,
    tail_scr,
    down_scr,
    sems,
):
    tokens = near_ref.shape[0]
    tiles, _, tile = taps_ref.shape
    tiles -= 1
    main = tiles * tile
    parts, cols, _ = down_scr.shape
    j = pl.program_id(0)

    def copies(n):
        rows = pl.ds(pl.multiple_of(order_ref[n] * cols, 128), cols)
        return (
            pltpu.make_async_copy(
                w_ref.at[rows, pl.ds(2 * main, main)],
                down_scr.at[n, :, pl.ds(0, main)],
                sems.at[2 * n],
            ),
            pltpu.make_async_copy(
                w_ref.at[rows, pl.ds(3 * main, 128)],
                down_scr.at[n, :, pl.ds(main, 128)],
                sems.at[2 * n + 1],
            ),
        )

    def hidden(gate, value, taps, rows):
        near, far = near_ref[rows, :], far_ref[rows, :]
        one = pltpu.roll(gate, 1, 0)[HALO:, :]
        two = pltpu.roll(gate, 2, 0)[HALO:, :]
        conv = (
            taps[2:3, :] * gate[HALO:, :]
            + taps[1:2, :] * (near * one)
            + taps[0:1, :] * (far * two)
        )
        scaled = 0.5 * conv
        return (scaled + scaled * jnp.tanh(scaled)) * value

    block = 96

    def finish(slot, at):
        for start in range(0, tokens, block):
            for half in range(0, tile, 128):
                lanes = slice(half, half + 128)
                done = hidden(
                    gate_scr[slot, start : start + block + HALO, lanes],
                    value_scr[slot, start + HALO : start + HALO + block, lanes],
                    taps_ref[at, :, lanes],
                    slice(start, start + block),
                )
                spot = at * tile + half
                if not isinstance(at, int):
                    spot = pl.multiple_of(spot, 128)
                h_ref[start : start + block, pl.ds(spot, 128)] = done.astype(BF16)

    def finish_tail():
        for start in range(0, tokens, block):
            part = tail_scr[start : start + block + HALO, :]
            lane = lax.broadcasted_iota(jnp.int32, (block, 128), 1)
            mine = (lane >= 64) & (lane < 96)
            done = hidden(
                pltpu.roll(part, 64, 1),
                pltpu.roll(part, 32, 1)[HALO:, :],
                taps_ref[tiles, :, 0:128],
                slice(start, start + block),
            )
            h_ref[start : start + block, main:] = jnp.where(mine, done, 0.0).astype(BF16)

    def project(slot):
        gate_scr[slot] = jnp.dot(x_ref[...], wg_ref[...], preferred_element_type=F32)
        value_scr[slot] = jnp.dot(x_ref[...], wv_ref[...], preferred_element_type=F32)

    def product(n, cuts):
        total = None
        for cut in cuts:
            term = lax.dot_general(
                h_ref[:, cut],
                down_scr[n, :, cut],
                (((1,), (1,)), ((), ())),
                preferred_element_type=F32,
            )
            total = term if total is None else total + term
        return total.astype(BF16)

    @pl.when(j == 0)
    def _():
        for n in range(parts):
            for copy in copies(n):
                copy.start()
        tail_scr[...] = jnp.dot(x_ref[...], wt_ref[...], preferred_element_type=F32)
        project(0)

    @pl.when(j == 1)
    def _():
        project(1)
        finish_tail()
        finish(0, 0)

    @pl.when((j > 1) & (j < tiles))
    def _():
        project(j % 2)
        finish((j - 1) % 2, j - 1)

    @pl.when(j >= tiles)
    def _():
        for k in range(2):
            for copy in copies(2 * (j - tiles) + k):
                copy.wait()

    @pl.when(j == tiles)
    def _():
        finish((tiles - 1) % 2, tiles - 1)
        known = main - tile
        cuts = (slice(0, known), slice(main, main + 128), slice(known, main))
        swap_ref[0] = product(0, cuts)
        own_ref[0] = product(1, cuts)

    @pl.when(j > tiles)
    def _():
        n = 2 * (j - tiles)
        swap_ref[0] = product(n, (slice(None),))
        own_ref[0] = product(n + 1, (slice(None),))


def down_kernel(order_ref, h_ref, wa_ref, wb_ref, ta_ref, tb_ref, swap_ref, own_ref):
    main = wa_ref.shape[1]
    contract = (((1,), (1,)), ((), ()))
    for ref, w_ref, t_ref in ((swap_ref, wa_ref, ta_ref), (own_ref, wb_ref, tb_ref)):
        ref[0] = (
            lax.dot_general(h_ref[:, :main], w_ref[...], contract, preferred_element_type=F32)
            + lax.dot_general(h_ref[:, main:], t_ref[...], contract, preferred_element_type=F32)
        ).astype(BF16)


def added(*terms):
    total = terms[0].astype(F32)
    for term in terms[1:]:
        total = total + term.astype(F32)
    return total


def shifted(value, by):
    ring = lax.axis_size("y")
    return lax.ppermute(value, "y", [(i, (i + by) % ring) for i in range(ring)])


def swapped(value):
    return lax.ppermute(value, "c", [(0, 1), (1, 0)])


def summed_over_tp(swap, own, last):
    other = swapped(swap)
    far, up, down = (added(own[k], other[k]) for k in range(3))
    half = far.shape[0] // 2
    far = far.astype(BF16)
    far_up, far_down = shifted(far[:half], 1), shifted(far[half:], -1)
    below = shifted(up[half:].astype(BF16), 1)
    above = shifted(down[:half].astype(BF16), -1)
    swap, own = last()
    near = added(own, swapped(swap))
    up = (up[:half] + far_up.astype(F32)).astype(BF16)
    down = (down[half:] + far_down.astype(F32)).astype(BF16)
    up, down = shifted(up, 1), shifted(down, -1)
    return added(near[:half], up, above), added(near[half:], below, down)


def gathered_over_tp(own):
    half = own.shape[0] // 2
    below, above = shifted(own, 1), shifted(own, -1)
    far = jnp.concatenate([shifted(below[:half], 1), shifted(above[half:], -1)], axis=0)
    mine = [own, below, above, far]
    return mine + [swapped(part) for part in mine]


def shape(dims, dtype):
    return jax.ShapeDtypeStruct(dims, dtype)


def whole(dims):
    return pl.BlockSpec(dims, lambda *_: (0,) * len(dims))


def layer(
    resid,
    query,
    keys,
    values,
    out_gate,
    in_gate,
    forget,
    doc_ids,
    head_gain,
    w_out,
    ffn_gain,
    w_gate,
    w_value,
    conv_taps,
    w_down,
):
    tokens, width = query.shape
    cols = resid.shape[1]
    model = w_out.shape[1]
    hidden = w_gate.shape[1]
    main = hidden // 128 * 128
    spare = hidden - main
    packed = pl.pallas_call(
        pack_kernel,
        out_shape=shape((w_gate.shape[0], 3 * main + 128), BF16),
        name="pack",
    )(w_gate, w_value, w_down.T)
    weights = lax.all_gather(packed, SP, axis=0, tiled=True)
    tile = 256
    tiles = main // tile
    spot = 2 * spare
    taps = jnp.concatenate(
        [
            jnp.swapaxes(conv_taps[:, :main].reshape(3, tiles, tile), 0, 1),
            jnp.pad(conv_taps[:, main:], ((0, 0), (spot, tile - spot - spare)))[None],
        ],
        axis=0,
    )

    pay, rows, cols_aux = pl.pallas_call(
        state_kernel,
        out_shape=(
            shape((DH + 16, width), BF16),
            shape((8, tokens), F32),
            shape((tokens, 8), F32),
        ),
        scratch_shapes=[pltpu.VMEM((8, tokens), F32)],
        name="state",
    )(keys, values, in_gate, forget, doc_ids.reshape(1, tokens))
    count = lax.axis_size(SP)
    reach = -(-(DOC_MAX - 1) // tokens)
    pays = [
        lax.ppermute(pay, SP, [(i, i + k) for i in range(count - k)]) for k in range(1, reach + 1)
    ]
    local = pl.pallas_call(
        local_kernel,
        out_shape=shape((tokens, width), F32),
        name="local",
    )(query, keys, values, rows, cols_aux)
    chip, core = lax.axis_index("y"), lax.axis_index("c")
    ring, cores = lax.axis_size("y"), lax.axis_size("c")
    order = (chip + jnp.array([2, 2, 1, 1, 3, 3, 0, 0], jnp.int32)) % ring * cores + (
        core ^ jnp.array([1, 0] * ring, jnp.int32)
    )
    swap, own, near, far_flags = pl.pallas_call(
        mix_kernel,
        grid_spec=pltpu.PrefetchScalarGridSpec(
            num_scalar_prefetch=1,
            grid=(ring,),
            in_specs=[
                whole((tokens, width)),
                whole((tokens, width)),
                whole((tokens, width)),
                whole((8, tokens)),
                whole((tokens, 8)),
                whole((1, width)),
                pl.BlockSpec((width, cols), lambda j, order: (0, order[2 * j])),
                pl.BlockSpec((width, cols), lambda j, order: (0, order[2 * j + 1])),
                *[whole((DH + 16, width)) for _ in pays],
            ],
            out_specs=(
                pl.BlockSpec((1, tokens, cols), lambda j, order: (j, 0, 0)),
                pl.BlockSpec((1, tokens, cols), lambda j, order: (j, 0, 0)),
                whole((tokens, 128)),
                whole((tokens, 128)),
            ),
            scratch_shapes=[pltpu.VMEM((tokens, width), BF16)],
        ),
        out_shape=(
            shape((ring, tokens, cols), BF16),
            shape((ring, tokens, cols), BF16),
            shape((tokens, 128), F32),
            shape((tokens, 128), F32),
        ),
        name="mix",
    )(order, query, out_gate, local, rows, cols_aux, head_gain.reshape(1, width), w_out, w_out, *pays)
    attended = summed_over_tp(swap[:3], own[:3], lambda: (swap[3], own[3]))
    residual_own = resid.astype(F32) + jnp.concatenate(attended, axis=0)
    pieces = gathered_over_tp(residual_own.astype(BF16))
    places = (chip + jnp.array([0, ring - 1, 1, 2] * 2, jnp.int32)) % ring * cores + (
        core ^ jnp.array([0] * ring + [1] * ring, jnp.int32)
    )
    block = 96
    normed, send = pl.pallas_call(
        norm_kernel,
        grid_spec=pltpu.PrefetchScalarGridSpec(
            num_scalar_prefetch=1,
            grid=(tokens // block,),
            in_specs=[
                *[pl.BlockSpec((block, cols), lambda i, places: (i, 0)) for _ in pieces],
                whole((1, model)),
            ],
            out_specs=(whole((tokens + HALO, model)), whole((HALO, model))),
        ),
        out_shape=(shape((tokens + HALO, model), BF16), shape((HALO, model), BF16)),
        compiler_params=pltpu.CompilerParams(vmem_limit_bytes=40 * 2**20),
        name="norm",
    )(places, *pieces, ffn_gain.reshape(1, model))
    edge = lax.ppermute(send, SP, [(i, i + 1) for i in range(count - 1)])
    normed = lax.dynamic_update_slice(normed, edge, (0, 0))
    tail_at = 3 * main // 128
    sent = 2 * (ring - 1)
    hidden, swap, own = pl.pallas_call(
        mixer_kernel,
        grid_spec=pltpu.PrefetchScalarGridSpec(
            num_scalar_prefetch=1,
            grid=(tiles + ring - 1,),
            in_specs=[
                pl.BlockSpec(
                    (tokens + HALO, model), lambda j, order: (0, 0), pipeline_mode=pl.Buffered(1)
                ),
                whole((tokens, 128)),
                whole((tokens, 128)),
                whole((tiles + 1, 3, tile)),
                pl.BlockSpec((model, tile), lambda j, order: (0, jnp.minimum(j, tiles - 1))),
                pl.BlockSpec(
                    (model, tile), lambda j, order: (0, tiles + jnp.minimum(j, tiles - 1))
                ),
                pl.BlockSpec(
                    (model, 128), lambda j, order: (0, tail_at), pipeline_mode=pl.Buffered(1)
                ),
                pl.BlockSpec(memory_space=pl.ANY),
            ],
            out_specs=(
                whole((tokens, main + 128)),
                pl.BlockSpec(
                    (1, tokens, cols), lambda j, order: (jnp.maximum(j - tiles, 0), 0, 0)
                ),
                pl.BlockSpec(
                    (1, tokens, cols), lambda j, order: (jnp.maximum(j - tiles, 0), 0, 0)
                ),
            ),
            scratch_shapes=[
                pltpu.VMEM((2, tokens + HALO, tile), F32),
                pltpu.VMEM((2, tokens + HALO, tile), F32),
                pltpu.VMEM((tokens + HALO, 128), F32),
                pltpu.VMEM((sent, cols, main + 128), BF16),
                pltpu.SemaphoreType.DMA((2 * sent,)),
            ],
        ),
        out_shape=(
            shape((tokens, main + 128), BF16),
            shape((ring - 1, tokens, cols), BF16),
            shape((ring - 1, tokens, cols), BF16),
        ),
        compiler_params=pltpu.CompilerParams(vmem_limit_bytes=58 * 2**20),
        name="mixer",
    )(order, normed, near, far_flags, taps, *[weights] * 4)

    def last():
        def spot(k, col):
            return lambda j, order: (order[sent + k], col)

        one = shape((1, tokens, cols), BF16)
        swap, own = pl.pallas_call(
            down_kernel,
            grid_spec=pltpu.PrefetchScalarGridSpec(
                num_scalar_prefetch=1,
                grid=(1,),
                in_specs=[
                    whole((tokens, main + 128)),
                    pl.BlockSpec((cols, main), spot(0, 2)),
                    pl.BlockSpec((cols, main), spot(1, 2)),
                    pl.BlockSpec((cols, 128), spot(0, tail_at)),
                    pl.BlockSpec((cols, 128), spot(1, tail_at)),
                ],
                out_specs=(whole((1, tokens, cols)), whole((1, tokens, cols))),
            ),
            out_shape=(one, one),
            compiler_params=pltpu.CompilerParams(vmem_limit_bytes=40 * 2**20),
            name="down",
        )(order, hidden, *[weights] * 4)
        return swap[0], own[0]

    down = summed_over_tp(swap, own, last)
    return (residual_own + jnp.concatenate(down, axis=0)).astype(BF16)


def solution(mesh):
    torus = Mesh(mesh.devices.reshape(4, 4, 4, 2), ("z", "x", "y", "c"))
    placed = (
        P(SP, TP),
        P(SP, TP),
        P(SP, TP),
        P(SP, TP),
        P(SP, TP),
        P(TP, SP),
        P(TP, SP),
        P(SP),
        P(TP),
        P(TP, None),
        P(),
        P(SP, TP),
        P(SP, TP),
        P(None, TP),
        P(TP, SP),
    )
    return jax.shard_map(layer, mesh=torus, in_specs=placed, out_specs=P(SP, TP), check_vma=False)
```

```python
import jax
import jax.numpy as jnp
from jax import lax
from jax.experimental import pallas as pl
from jax.experimental.pallas import tpu as pltpu
from jax.sharding import Mesh
from jax.sharding import PartitionSpec as P


DH = 96
DOC_MAX = 3072
SP = ("z", "x")
TP = ("y", "c")
ABSENT = -1e30
HALO = 16
EPS = 1e-06
HEAD_FLOOR = 1.0
F32 = jnp.float32
BF16 = jnp.bfloat16


def in_first_head(shape):
    return lax.broadcasted_iota(jnp.int32, shape, len(shape) - 1) < DH


def pack_kernel(gate_ref, value_ref, down_ref, out_ref):
    rows, hidden = gate_ref.shape
    main = hidden // 128 * 128
    tails = []
    for k, ref in enumerate((gate_ref, value_ref, down_ref)):
        out_ref[:, k * main : (k + 1) * main] = ref[:, :main]
        tails.append(ref[:, main:])
    tails.append(jnp.zeros((rows, 128 - 3 * (hidden - main)), BF16))
    out_ref[:, 3 * main :] = jnp.concatenate(tails, axis=1)


def state_kernel(k_ref, v_ref, in_ref, forget_ref, doc_ref, pay_ref, row_ref, col_ref, scr):
    tokens, width = k_ref.shape
    lane = lax.broadcasted_iota(jnp.int32, (8, tokens), 1)
    doc = jnp.broadcast_to(doc_ref[...].astype(F32), (8, tokens))
    scr[...] = jnp.zeros_like(scr)
    scr[0:2, :] = forget_ref[...]
    raw = scr[...]
    total = jnp.minimum(raw, 0.0) - jnp.log1p(jnp.exp(-jnp.abs(raw)))
    step = 1
    while step < tokens:
        total = total + jnp.where(lane >= step, pltpu.roll(total, step, 1), 0.0)
        step *= 2
    scr[0:2, :] = in_ref[...]
    rest = scr[...] - total
    peak = rest
    step = 1
    while step < tokens:
        near = (lane >= step) & (pltpu.roll(doc, step, 1) == doc)
        peak = jnp.maximum(peak, jnp.where(near, pltpu.roll(peak, step, 1), ABSENT))
        step *= 2
    end_doc = doc[:, tokens - 1 : tokens]
    end_peak = peak[:, tokens - 1 : tokens]
    end_total = total[:, tokens - 1 : tokens]
    weight = jnp.where(doc == end_doc, jnp.exp(jnp.minimum(rest - end_peak, 0.0)), 0.0)
    row_ref[...] = jnp.zeros_like(row_ref)
    row_ref[0:2, :] = total[0:2, :]
    row_ref[2:4, :] = peak[0:2, :]
    row_ref[4:6, :] = weight[0:2, :]
    row_ref[6:7, :] = doc[0:1, :]
    scr[...] = row_ref[...]
    cols = scr[...].T
    col_ref[...] = cols
    row_ref[4:6, :] = rest[0:2, :]
    first = in_first_head((tokens, width))
    spread = jnp.where(first, cols[:, 4:5], cols[:, 5:6])
    weighted = (k_ref[...].astype(F32) * (spread * DH**-0.5)).astype(BF16)
    state = lax.dot_general(
        weighted, v_ref[...], (((0,), (0,)), ((), ())), preferred_element_type=F32
    )
    small = in_first_head((DH, width))
    pay_ref[0:DH, :] = jnp.where(small, state[0:DH, :], state[DH:, :]).astype(BF16)

    line = in_first_head((1, width))

    def spread_heads(x):
        return jnp.where(line, x[0:1, :], x[1:2, :])

    def split(x):
        high = x.astype(BF16).astype(F32)
        mid = (x - high).astype(BF16).astype(F32)
        return high, mid, x - high - mid

    lines = [
        *split(spread_heads(end_total + end_peak)),
        *split(spread_heads(end_total)),
        jnp.broadcast_to(end_doc[0:1, :] + 1.0, (1, width)),
        jnp.broadcast_to(doc[0:1, tokens - 2 : tokens - 1] + 1.0, (1, width)),
    ]
    place = lax.broadcasted_iota(jnp.int32, (16, width), 0)
    table = jnp.zeros((16, width), F32)
    for k, value in enumerate(lines):
        table = jnp.where(place == k, value, table)
    pay_ref[DH:, :] = table.astype(BF16)


def local_kernel(q_ref, k_ref, v_ref, row_ref, col_ref, out_ref):
    tokens, width = q_ref.shape
    block = 256
    for start in range(0, tokens, block):
        stop = start + block
        keys = k_ref[0:stop, :]
        vals = v_ref[0:stop, :]
        q = q_ref[start:stop, :]
        first = in_first_head((block, width))
        at = lax.broadcasted_iota(jnp.int32, (block, stop), 0) + start
        source = lax.broadcasted_iota(jnp.int32, (block, stop), 1)
        seen = (at >= source) & (row_ref[6:7, 0:stop] == col_ref[start:stop, 6:7])
        found = []
        for h in range(2):
            mine = jnp.where(first if h == 0 else jnp.logical_not(first), q, jnp.zeros_like(q))
            scores = lax.dot_general(
                mine, keys, (((1,), (1,)), ((), ())), preferred_element_type=F32
            )
            gap = row_ref[4 + h : 5 + h, 0:stop] - col_ref[start:stop, 2 + h : 3 + h]
            part = (scores * jnp.exp(jnp.where(seen, gap, ABSENT))).astype(BF16)
            found.append(jnp.dot(part, vals, preferred_element_type=F32))
        out_ref[start:stop, :] = jnp.where(first, found[0], found[1])


def mix_kernel(
    order_ref, q_ref, gate_ref, local_ref, row_ref, col_ref, gain_ref, w_ref, *refs
):
    w_own_ref, *pays = refs[:-5]
    swap_ref, own_out_ref, near_ref, far_ref, mix_ref = refs[-5:]
    tokens, width = q_ref.shape

    @pl.when(pl.program_id(0) == 0)
    def _():
        own = row_ref[6:7, 0:1] + 1.0
        behind = jnp.zeros((1, width), F32)
        peaks, goods = [], []
        for ref in pays:
            table = ref[DH:, :].astype(F32)
            good = table[6:7, :] == own
            peaks.append(
                jnp.where(good, table[0:1, :] + table[1:2, :] + table[2:3, :] + behind, ABSENT)
            )
            goods.append(good)
            behind = behind + (table[3:4, :] + table[4:5, :] + table[5:6, :])
        best = peaks[0]
        for value in peaks[1:]:
            best = jnp.maximum(best, value)
        state = jnp.zeros((DH, width), F32)
        for ref, value, good in zip(pays, peaks, goods):
            state = state + jnp.where(good, jnp.exp(value - best), 0.0) * ref[0:DH, :].astype(F32)
        small = in_first_head((DH, width))
        whole = jnp.concatenate(
            [jnp.where(small, state, 0.0), jnp.where(small, 0.0, state)], axis=0
        ).astype(BF16)
        carried = jnp.dot(q_ref[...], whole, preferred_element_type=F32)
        first = in_first_head((tokens, width))
        total = jnp.where(first, col_ref[:, 0:1], col_ref[:, 1:2])
        peak = total + jnp.where(first, col_ref[:, 2:3], col_ref[:, 3:4])
        inter = jnp.where(col_ref[:, 6:7] + 1.0 == own, total + best, ABSENT)
        top = jnp.maximum(peak, inter)
        memory = (
            jnp.exp(peak - top) * (local_ref[...] * DH**-0.5) + jnp.exp(inter - top) * carried
        )
        square = memory * memory
        mean_0 = jnp.sum(jnp.where(first, square, 0.0), axis=1, keepdims=True) / DH
        mean_1 = jnp.sum(jnp.where(first, 0.0, square), axis=1, keepdims=True) / DH
        norm = jnp.where(first, lax.rsqrt(mean_0 + HEAD_FLOOR), lax.rsqrt(mean_1 + HEAD_FLOOR))
        gate = gate_ref[...].astype(F32)
        mix_ref[...] = (memory * norm * gain_ref[...] * (1.0 / (1.0 + jnp.exp(-gate)))).astype(BF16)

        ids = pays[0][DH:, :].astype(F32)
        last, second = ids[6:7, 0:1], ids[7:8, 0:1]
        doc = jnp.broadcast_to(col_ref[:, 6:7], (tokens, 128)) + 1.0
        row = lax.broadcasted_iota(jnp.int32, (tokens, 128), 0)
        one = jnp.where(row == 0, last, pltpu.roll(doc, 1, 0))
        two = jnp.where(row == 0, second, jnp.where(row == 1, last, pltpu.roll(doc, 2, 0)))
        near_ref[...] = (one == doc).astype(F32)
        far_ref[...] = (two == doc).astype(F32)

    mix = mix_ref[...]
    swap_ref[0] = jnp.dot(mix, w_ref[...], preferred_element_type=F32).astype(BF16)
    own_out_ref[0] = jnp.dot(mix, w_own_ref[...], preferred_element_type=F32).astype(BF16)


def norm_kernel(order_ref, *refs):
    pieces, (gain_ref, out_ref, send_ref) = refs[:-3], refs[-3:]
    tokens, cols = pieces[0].shape
    model = out_ref.shape[1]
    i = pl.program_id(0)
    square = jnp.zeros((tokens, cols), F32)
    for ref in pieces:
        r = ref[...].astype(F32)
        square = square + r * r
    mean = jnp.sum(square, axis=1, keepdims=True) / model
    scale = lax.rsqrt(mean + EPS)
    rows = pl.ds(pl.multiple_of(HALO + i * tokens, 16), tokens)
    for p, ref in enumerate(pieces):
        cut = pl.ds(pl.multiple_of(order_ref[p] * cols, 128), cols)
        done = (ref[...].astype(F32) * scale * gain_ref[0:1, cut]).astype(BF16)
        out_ref[rows, cut] = done
        send_ref[:, cut] = done[tokens - HALO :, :]


def mixer_kernel(
    order_ref,
    x_ref,
    near_ref,
    far_ref,
    taps_ref,
    wg_ref,
    wv_ref,
    wt_ref,
    w_ref,
    h_ref,
    swap_ref,
    own_ref,
    gate_scr,
    value_scr,
    tail_scr,
    down_scr,
    sems,
):
    tokens = near_ref.shape[0]
    tiles, _, tile = taps_ref.shape
    tiles -= 1
    main = tiles * tile
    pairs, cols = down_scr.shape[0], down_scr.shape[1] // 2
    j = pl.program_id(0)

    def copies(n):
        rows = pl.ds(pl.multiple_of(order_ref[n] * cols, 128), cols)
        spot = down_scr.at[n // 2, pl.ds(n % 2 * cols, cols)]
        return (
            pltpu.make_async_copy(
                w_ref.at[rows, pl.ds(2 * main, main)],
                spot.at[:, pl.ds(0, main)],
                sems.at[2 * n],
            ),
            pltpu.make_async_copy(
                w_ref.at[rows, pl.ds(3 * main, 128)],
                spot.at[:, pl.ds(main, 128)],
                sems.at[2 * n + 1],
            ),
        )

    def hidden(gate, value, taps, rows):
        near, far = near_ref[rows, :], far_ref[rows, :]
        one = pltpu.roll(gate, 1, 0)[HALO:, :]
        two = pltpu.roll(gate, 2, 0)[HALO:, :]
        conv = (
            taps[2:3, :] * gate[HALO:, :]
            + taps[1:2, :] * (near * one)
            + taps[0:1, :] * (far * two)
        )
        scaled = 0.5 * conv
        return (scaled + scaled * jnp.tanh(scaled)) * value

    block = 96

    def finish(slot, at):
        for start in range(0, tokens, block):
            for half in range(0, tile, 128):
                lanes = slice(half, half + 128)
                done = hidden(
                    gate_scr[slot, start : start + block + HALO, lanes],
                    value_scr[slot, start + HALO : start + HALO + block, lanes],
                    taps_ref[at, :, lanes],
                    slice(start, start + block),
                )
                spot = at * tile + half
                if not isinstance(at, int):
                    spot = pl.multiple_of(spot, 128)
                h_ref[start : start + block, pl.ds(spot, 128)] = done.astype(BF16)

    def finish_tail():
        for start in range(0, tokens, block):
            part = tail_scr[start : start + block + HALO, :]
            lane = lax.broadcasted_iota(jnp.int32, (block, 128), 1)
            mine = (lane >= 64) & (lane < 96)
            done = hidden(
                pltpu.roll(part, 64, 1),
                pltpu.roll(part, 32, 1)[HALO:, :],
                taps_ref[tiles, :, 0:128],
                slice(start, start + block),
            )
            h_ref[start : start + block, main:] = jnp.where(mine, done, 0.0).astype(BF16)

    def project(slot):
        gate_scr[slot] = jnp.dot(x_ref[...], wg_ref[...], preferred_element_type=F32)
        value_scr[slot] = jnp.dot(x_ref[...], wv_ref[...], preferred_element_type=F32)

    def product(n, cuts):
        total = None
        for cut in cuts:
            term = lax.dot_general(
                h_ref[:, cut],
                down_scr[n, :, cut],
                (((1,), (1,)), ((), ())),
                preferred_element_type=F32,
            )
            total = term if total is None else total + term
        return total.astype(BF16)

    @pl.when(j == 0)
    def _():
        for n in range(2 * pairs):
            for copy in copies(n):
                copy.start()
        tail_scr[...] = jnp.dot(x_ref[...], wt_ref[...], preferred_element_type=F32)
        project(0)

    @pl.when(j == 1)
    def _():
        project(1)
        finish_tail()
        finish(0, 0)

    @pl.when((j > 1) & (j < tiles))
    def _():
        project(j % 2)
        finish((j - 1) % 2, j - 1)

    @pl.when(j == tiles)
    def _():
        finish((tiles - 1) % 2, tiles - 1)
        for n in range(2):
            for copy in copies(n):
                copy.wait()
        known = main - tile
        both = product(0, (slice(0, known), slice(main, main + 128), slice(known, main)))
        swap_ref[0], own_ref[0] = both[:, :cols], both[:, cols:]

    @pl.when(j > tiles)
    def _():
        for n in range(2, 4):
            for copy in copies(n):
                copy.wait()
        both = product(1, (slice(None),))
        swap_ref[1], swap_ref[2] = both[:, :cols], both[:, cols:]


def two_parts(h_ref, wa_ref, wb_ref, ta_ref, tb_ref):
    main = wa_ref.shape[1]
    contract = (((1,), (1,)), ((), ()))
    main_w = jnp.concatenate([wa_ref[...], wb_ref[...]], axis=0)
    tail_w = jnp.concatenate([ta_ref[...], tb_ref[...]], axis=0)
    both = lax.dot_general(
        h_ref[:, :main], main_w, contract, preferred_element_type=F32
    ) + lax.dot_general(h_ref[:, main:], tail_w, contract, preferred_element_type=F32)
    cols = wa_ref.shape[0]
    return both[:, :cols], both[:, cols:]


def side_kernel(order_ref, h_ref, wa_ref, wb_ref, ta_ref, tb_ref, a_ref, b_ref, up_ref, down_ref):
    up, down = two_parts(h_ref, wa_ref, wb_ref, ta_ref, tb_ref)
    up_ref[...] = (up + a_ref[0].astype(F32)).astype(BF16)
    down_ref[...] = (down + b_ref[0].astype(F32)).astype(BF16)


def down_kernel(order_ref, h_ref, wa_ref, wb_ref, ta_ref, tb_ref, swap_ref, own_ref):
    swap, own = two_parts(h_ref, wa_ref, wb_ref, ta_ref, tb_ref)
    swap_ref[...] = swap.astype(BF16)
    own_ref[...] = own.astype(BF16)


def added(*terms):
    total = terms[0].astype(F32)
    for term in terms[1:]:
        total = total + term.astype(F32)
    return total


def shifted(value, by):
    ring = lax.axis_size("y")
    return lax.ppermute(value, "y", [(i, (i + by) % ring) for i in range(ring)])


def swapped(value):
    return lax.ppermute(value, "c", [(0, 1), (1, 0)])


def summed_over_tp(swap, own, sides, last):
    other = swapped(swap)
    far = added(own, other[0]).astype(BF16)
    half = far.shape[0] // 2
    far_up, far_down = shifted(far[:half], 1), shifted(far[half:], -1)
    up, down = sides(other)
    below, above = shifted(up[half:], 1), shifted(down[:half], -1)
    up = added(up[:half], far_up).astype(BF16)
    down = added(down[half:], far_down).astype(BF16)
    up, down = shifted(up, 1), shifted(down, -1)
    swap, own = last()
    near = added(own, swapped(swap))
    return added(near[:half], up, above), added(near[half:], below, down)


def gathered_over_tp(own):
    half = own.shape[0] // 2
    below, above = shifted(own, 1), shifted(own, -1)
    far = jnp.concatenate([shifted(below[:half], 1), shifted(above[half:], -1)], axis=0)
    mine = [own, below, above, far]
    return mine + [swapped(part) for part in mine]


def shape(dims, dtype):
    return jax.ShapeDtypeStruct(dims, dtype)


def whole(dims):
    return pl.BlockSpec(dims, lambda *_: (0,) * len(dims))


def layer(
    resid,
    query,
    keys,
    values,
    out_gate,
    in_gate,
    forget,
    doc_ids,
    head_gain,
    w_out,
    ffn_gain,
    w_gate,
    w_value,
    conv_taps,
    w_down,
):
    tokens, width = query.shape
    cols = resid.shape[1]
    model = w_out.shape[1]
    hidden = w_gate.shape[1]
    main = hidden // 128 * 128
    spare = hidden - main
    packed = pl.pallas_call(
        pack_kernel,
        out_shape=shape((w_gate.shape[0], 3 * main + 128), BF16),
        name="pack",
    )(w_gate, w_value, w_down.T)
    weights = lax.all_gather(packed, SP, axis=0, tiled=True)
    tile = 256
    tiles = main // tile
    spot = 2 * spare
    taps = jnp.concatenate(
        [
            jnp.swapaxes(conv_taps[:, :main].reshape(3, tiles, tile), 0, 1),
            jnp.pad(conv_taps[:, main:], ((0, 0), (spot, tile - spot - spare)))[None],
        ],
        axis=0,
    )

    pay, rows, cols_aux = pl.pallas_call(
        state_kernel,
        out_shape=(
            shape((DH + 16, width), BF16),
            shape((8, tokens), F32),
            shape((tokens, 8), F32),
        ),
        scratch_shapes=[pltpu.VMEM((8, tokens), F32)],
        name="state",
    )(keys, values, in_gate, forget, doc_ids.reshape(1, tokens))
    count = lax.axis_size(SP)
    reach = -(-(DOC_MAX - 1) // tokens)
    pays = [
        lax.ppermute(pay, SP, [(i, i + k) for i in range(count - k)]) for k in range(1, reach + 1)
    ]
    local = pl.pallas_call(
        local_kernel,
        out_shape=shape((tokens, width), F32),
        name="local",
    )(query, keys, values, rows, cols_aux)
    chip, core = lax.axis_index("y"), lax.axis_index("c")
    ring, cores = lax.axis_size("y"), lax.axis_size("c")
    order = (chip + jnp.array([2, 2, 1, 1, 3, 3, 0, 0], jnp.int32)) % ring * cores + (
        core ^ jnp.array([1, 0] * ring, jnp.int32)
    )
    swap, own, near, far_flags = pl.pallas_call(
        mix_kernel,
        grid_spec=pltpu.PrefetchScalarGridSpec(
            num_scalar_prefetch=1,
            grid=(ring,),
            in_specs=[
                whole((tokens, width)),
                whole((tokens, width)),
                whole((tokens, width)),
                whole((8, tokens)),
                whole((tokens, 8)),
                whole((1, width)),
                pl.BlockSpec((width, cols), lambda j, order: (0, order[2 * j])),
                pl.BlockSpec((width, cols), lambda j, order: (0, order[2 * j + 1])),
                *[whole((DH + 16, width)) for _ in pays],
            ],
            out_specs=(
                pl.BlockSpec((1, tokens, cols), lambda j, order: (j, 0, 0)),
                pl.BlockSpec((1, tokens, cols), lambda j, order: (j, 0, 0)),
                whole((tokens, 128)),
                whole((tokens, 128)),
            ),
            scratch_shapes=[pltpu.VMEM((tokens, width), BF16)],
        ),
        out_shape=(
            shape((ring, tokens, cols), BF16),
            shape((ring, tokens, cols), BF16),
            shape((tokens, 128), F32),
            shape((tokens, 128), F32),
        ),
        name="mix",
    )(order, query, out_gate, local, rows, cols_aux, head_gain.reshape(1, width), w_out, w_out, *pays)
    attended = summed_over_tp(
        swap[:3],
        own[0],
        lambda other: tuple(added(own[k], other[k]).astype(BF16) for k in (1, 2)),
        lambda: (swap[3], own[3]),
    )
    residual_own = resid.astype(F32) + jnp.concatenate(attended, axis=0)
    pieces = gathered_over_tp(residual_own.astype(BF16))
    places = (chip + jnp.array([0, ring - 1, 1, 2] * 2, jnp.int32)) % ring * cores + (
        core ^ jnp.array([0] * ring + [1] * ring, jnp.int32)
    )
    block = 96
    normed, send = pl.pallas_call(
        norm_kernel,
        grid_spec=pltpu.PrefetchScalarGridSpec(
            num_scalar_prefetch=1,
            grid=(tokens // block,),
            in_specs=[
                *[pl.BlockSpec((block, cols), lambda i, places: (i, 0)) for _ in pieces],
                whole((1, model)),
            ],
            out_specs=(whole((tokens + HALO, model)), whole((HALO, model))),
        ),
        out_shape=(shape((tokens + HALO, model), BF16), shape((HALO, model), BF16)),
        compiler_params=pltpu.CompilerParams(vmem_limit_bytes=40 * 2**20),
        name="norm",
    )(places, *pieces, ffn_gain.reshape(1, model))
    edge = lax.ppermute(send, SP, [(i, i + 1) for i in range(count - 1)])
    normed = lax.dynamic_update_slice(normed, edge, (0, 0))
    tail_at = 3 * main // 128
    order = (chip + jnp.array([2, 2, 1, 3, 1, 3, 0, 0], jnp.int32)) % ring * cores + (
        core ^ jnp.array([1, 0, 1, 1, 0, 0, 1, 0], jnp.int32)
    )
    hidden, swap, own = pl.pallas_call(
        mixer_kernel,
        grid_spec=pltpu.PrefetchScalarGridSpec(
            num_scalar_prefetch=1,
            grid=(tiles + 2,),
            in_specs=[
                pl.BlockSpec(
                    (tokens + HALO, model), lambda j, order: (0, 0), pipeline_mode=pl.Buffered(1)
                ),
                whole((tokens, 128)),
                whole((tokens, 128)),
                whole((tiles + 1, 3, tile)),
                pl.BlockSpec((model, tile), lambda j, order: (0, jnp.minimum(j, tiles - 1))),
                pl.BlockSpec(
                    (model, tile), lambda j, order: (0, tiles + jnp.minimum(j, tiles - 1))
                ),
                pl.BlockSpec(
                    (model, 128), lambda j, order: (0, tail_at), pipeline_mode=pl.Buffered(1)
                ),
                pl.BlockSpec(memory_space=pl.ANY),
            ],
            out_specs=(
                whole((tokens, main + 128)),
                whole((3, tokens, cols)),
                whole((1, tokens, cols)),
            ),
            scratch_shapes=[
                pltpu.VMEM((2, tokens + HALO, tile), F32),
                pltpu.VMEM((2, tokens + HALO, tile), F32),
                pltpu.VMEM((tokens + HALO, 128), F32),
                pltpu.VMEM((2, 2 * cols, main + 128), BF16),
                pltpu.SemaphoreType.DMA((8,)),
            ],
        ),
        out_shape=(
            shape((tokens, main + 128), BF16),
            shape((3, tokens, cols), BF16),
            shape((1, tokens, cols), BF16),
        ),
        compiler_params=pltpu.CompilerParams(vmem_limit_bytes=58 * 2**20),
        name="mixer",
    )(order, normed, near, far_flags, taps, *[weights] * 4)

    def more(kernel, at, given, specs):
        def spot(k, col):
            return lambda j, order: (order[at + k], col)

        one = shape((tokens, cols), BF16)
        return pl.pallas_call(
            kernel,
            grid_spec=pltpu.PrefetchScalarGridSpec(
                num_scalar_prefetch=1,
                grid=(1,),
                in_specs=[
                    whole((tokens, main + 128)),
                    pl.BlockSpec((cols, main), spot(0, 2)),
                    pl.BlockSpec((cols, main), spot(1, 2)),
                    pl.BlockSpec((cols, 128), spot(0, tail_at)),
                    pl.BlockSpec((cols, 128), spot(1, tail_at)),
                    *specs,
                ],
                out_specs=(whole((tokens, cols)), whole((tokens, cols))),
            ),
            out_shape=(one, one),
            compiler_params=pltpu.CompilerParams(vmem_limit_bytes=40 * 2**20),
        )(order, hidden, *[weights] * 4, *given)

    down = summed_over_tp(
        swap,
        own[0],
        lambda other: more(
            side_kernel,
            4,
            (other, other),
            [pl.BlockSpec((1, tokens, cols), lambda j, order, k=k: (k, 0, 0)) for k in (1, 2)],
        ),
        lambda: more(down_kernel, 6, (), []),
    )
    return (residual_own + jnp.concatenate(down, axis=0)).astype(BF16)


def solution(mesh):
    torus = Mesh(mesh.devices.reshape(4, 4, 4, 2), ("z", "x", "y", "c"))
    placed = (
        P(SP, TP),
        P(SP, TP),
        P(SP, TP),
        P(SP, TP),
        P(SP, TP),
        P(TP, SP),
        P(TP, SP),
        P(SP),
        P(TP),
        P(TP, None),
        P(),
        P(SP, TP),
        P(SP, TP),
        P(None, TP),
        P(TP, SP),
    )
    return jax.shard_map(layer, mesh=torus, in_specs=placed, out_specs=P(SP, TP), check_vma=False)
```

```python
import jax
import jax.numpy as jnp
from jax import lax
from jax.experimental import pallas as pl
from jax.experimental.pallas import tpu as pltpu
from jax.sharding import Mesh
from jax.sharding import PartitionSpec as P


DH = 96
DOC_MAX = 3072
SP = ("z", "x")
TP = ("y", "c")
ABSENT = -1e30
HALO = 16
EPS = 1e-06
HEAD_FLOOR = 1.0
F32 = jnp.float32
BF16 = jnp.bfloat16


def in_first_head(shape):
    return lax.broadcasted_iota(jnp.int32, shape, len(shape) - 1) < DH


def pack_kernel(gate_ref, value_ref, down_ref, out_ref, tails, last, sems):
    rows, hidden = gate_ref.shape
    spare = tails.shape[2]
    main = hidden - spare
    ends, mains = [], []
    for k, ref in enumerate((gate_ref, value_ref, down_ref)):
        ends.append(
            pltpu.make_async_copy(ref.at[:, pl.ds(main, spare)], tails.at[k], sems.at[k])
        )
        mains.append(
            pltpu.make_async_copy(
                ref.at[:, pl.ds(0, main)], out_ref.at[:, pl.ds(k * main, main)], sems.at[3 + k]
            )
        )
    for copy in ends + mains:
        copy.start()
    for copy in ends:
        copy.wait()
    last[...] = jnp.concatenate(
        [tails[0], tails[1], tails[2], jnp.zeros((rows, 128 - 3 * spare), BF16)], axis=1
    )
    end = pltpu.make_async_copy(last, out_ref.at[:, pl.ds(3 * main, 128)], sems.at[6])
    end.start()
    for copy in mains:
        copy.wait()
    end.wait()


def state_kernel(k_ref, v_ref, in_ref, forget_ref, doc_ref, pay_ref, row_ref, col_ref, scr):
    tokens, width = k_ref.shape
    lane = lax.broadcasted_iota(jnp.int32, (8, tokens), 1)
    doc = jnp.broadcast_to(doc_ref[...].astype(F32), (8, tokens))
    scr[...] = jnp.zeros_like(scr)
    scr[0:2, :] = forget_ref[...]
    raw = scr[...]
    total = jnp.minimum(raw, 0.0) - jnp.log1p(jnp.exp(-jnp.abs(raw)))
    step = 1
    while step < tokens:
        total = total + jnp.where(lane >= step, pltpu.roll(total, step, 1), 0.0)
        step *= 2
    scr[0:2, :] = in_ref[...]
    rest = scr[...] - total
    peak = rest
    step = 1
    while step < tokens:
        near = (lane >= step) & (pltpu.roll(doc, step, 1) == doc)
        peak = jnp.maximum(peak, jnp.where(near, pltpu.roll(peak, step, 1), ABSENT))
        step *= 2
    end_doc = doc[:, tokens - 1 : tokens]
    end_peak = peak[:, tokens - 1 : tokens]
    end_total = total[:, tokens - 1 : tokens]
    weight = jnp.where(doc == end_doc, jnp.exp(jnp.minimum(rest - end_peak, 0.0)), 0.0)
    row_ref[...] = jnp.zeros_like(row_ref)
    row_ref[0:2, :] = total[0:2, :]
    row_ref[2:4, :] = peak[0:2, :]
    row_ref[4:6, :] = weight[0:2, :]
    row_ref[6:7, :] = doc[0:1, :]
    scr[...] = row_ref[...]
    cols = scr[...].T
    col_ref[...] = cols
    row_ref[4:6, :] = rest[0:2, :]
    first = in_first_head((tokens, width))
    spread = jnp.where(first, cols[:, 4:5], cols[:, 5:6])
    weighted = (k_ref[...].astype(F32) * (spread * DH**-0.5)).astype(BF16)
    state = lax.dot_general(
        weighted, v_ref[...], (((0,), (0,)), ((), ())), preferred_element_type=F32
    )
    small = in_first_head((DH, width))
    pay_ref[0:DH, :] = jnp.where(small, state[0:DH, :], state[DH:, :]).astype(BF16)

    line = in_first_head((1, width))

    def spread_heads(x):
        return jnp.where(line, x[0:1, :], x[1:2, :])

    def split(x):
        high = x.astype(BF16).astype(F32)
        mid = (x - high).astype(BF16).astype(F32)
        return high, mid, x - high - mid

    lines = [
        *split(spread_heads(end_total + end_peak)),
        *split(spread_heads(end_total)),
        jnp.broadcast_to(end_doc[0:1, :] + 1.0, (1, width)),
        jnp.broadcast_to(doc[0:1, tokens - 2 : tokens - 1] + 1.0, (1, width)),
    ]
    place = lax.broadcasted_iota(jnp.int32, (16, width), 0)
    table = jnp.zeros((16, width), F32)
    for k, value in enumerate(lines):
        table = jnp.where(place == k, value, table)
    pay_ref[DH:, :] = table.astype(BF16)


def local_kernel(q_ref, k_ref, v_ref, row_ref, col_ref, out_ref):
    tokens, width = q_ref.shape
    block = 256
    for start in range(0, tokens, block):
        stop = start + block
        keys = k_ref[0:stop, :]
        vals = v_ref[0:stop, :]
        q = q_ref[start:stop, :]
        first = in_first_head((block, width))
        at = lax.broadcasted_iota(jnp.int32, (block, stop), 0) + start
        source = lax.broadcasted_iota(jnp.int32, (block, stop), 1)
        seen = (at >= source) & (row_ref[6:7, 0:stop] == col_ref[start:stop, 6:7])
        found = []
        for h in range(2):
            mine = jnp.where(first if h == 0 else jnp.logical_not(first), q, jnp.zeros_like(q))
            scores = lax.dot_general(
                mine, keys, (((1,), (1,)), ((), ())), preferred_element_type=F32
            )
            gap = row_ref[4 + h : 5 + h, 0:stop] - col_ref[start:stop, 2 + h : 3 + h]
            part = (scores * jnp.exp(jnp.where(seen, gap, ABSENT))).astype(BF16)
            found.append(jnp.dot(part, vals, preferred_element_type=F32))
        out_ref[start:stop, :] = jnp.where(first, found[0], found[1])


def mix_kernel(
    order_ref, q_ref, gate_ref, local_ref, row_ref, col_ref, gain_ref, w_ref, *refs
):
    w_own_ref, *pays = refs[:-5]
    swap_ref, own_out_ref, near_ref, far_ref, mix_ref = refs[-5:]
    tokens, width = q_ref.shape

    @pl.when(pl.program_id(0) == 0)
    def _():
        own = row_ref[6:7, 0:1] + 1.0
        behind = jnp.zeros((1, width), F32)
        peaks, goods = [], []
        for ref in pays:
            table = ref[DH:, :].astype(F32)
            good = table[6:7, :] == own
            peaks.append(
                jnp.where(good, table[0:1, :] + table[1:2, :] + table[2:3, :] + behind, ABSENT)
            )
            goods.append(good)
            behind = behind + (table[3:4, :] + table[4:5, :] + table[5:6, :])
        best = peaks[0]
        for value in peaks[1:]:
            best = jnp.maximum(best, value)
        state = jnp.zeros((DH, width), F32)
        for ref, value, good in zip(pays, peaks, goods):
            state = state + jnp.where(good, jnp.exp(value - best), 0.0) * ref[0:DH, :].astype(F32)
        small = in_first_head((DH, width))
        whole = jnp.concatenate(
            [jnp.where(small, state, 0.0), jnp.where(small, 0.0, state)], axis=0
        ).astype(BF16)
        carried = jnp.dot(q_ref[...], whole, preferred_element_type=F32)
        first = in_first_head((tokens, width))
        total = jnp.where(first, col_ref[:, 0:1], col_ref[:, 1:2])
        peak = total + jnp.where(first, col_ref[:, 2:3], col_ref[:, 3:4])
        inter = jnp.where(col_ref[:, 6:7] + 1.0 == own, total + best, ABSENT)
        top = jnp.maximum(peak, inter)
        memory = (
            jnp.exp(peak - top) * (local_ref[...] * DH**-0.5) + jnp.exp(inter - top) * carried
        )
        square = memory * memory
        mean_0 = jnp.sum(jnp.where(first, square, 0.0), axis=1, keepdims=True) / DH
        mean_1 = jnp.sum(jnp.where(first, 0.0, square), axis=1, keepdims=True) / DH
        norm = jnp.where(first, lax.rsqrt(mean_0 + HEAD_FLOOR), lax.rsqrt(mean_1 + HEAD_FLOOR))
        gate = gate_ref[...].astype(F32)
        mix_ref[...] = (memory * norm * gain_ref[...] * (1.0 / (1.0 + jnp.exp(-gate)))).astype(BF16)

        ids = pays[0][DH:, :].astype(F32)
        last, second = ids[6:7, 0:1], ids[7:8, 0:1]
        doc = jnp.broadcast_to(col_ref[:, 6:7], (tokens, 128)) + 1.0
        row = lax.broadcasted_iota(jnp.int32, (tokens, 128), 0)
        one = jnp.where(row == 0, last, pltpu.roll(doc, 1, 0))
        two = jnp.where(row == 0, second, jnp.where(row == 1, last, pltpu.roll(doc, 2, 0)))
        near_ref[...] = (one == doc).astype(F32)
        far_ref[...] = (two == doc).astype(F32)

    mix = mix_ref[...]
    swap_ref[0] = jnp.dot(mix, w_ref[...], preferred_element_type=F32).astype(BF16)
    own_out_ref[0] = jnp.dot(mix, w_own_ref[...], preferred_element_type=F32).astype(BF16)


def norm_kernel(order_ref, *refs):
    pieces, (gain_ref, out_ref, send_ref) = refs[:-3], refs[-3:]
    tokens, cols = pieces[0].shape
    model = out_ref.shape[1]
    i = pl.program_id(0)
    square = jnp.zeros((tokens, cols), F32)
    for ref in pieces:
        r = ref[...].astype(F32)
        square = square + r * r
    mean = jnp.sum(square, axis=1, keepdims=True) / model
    scale = lax.rsqrt(mean + EPS)
    rows = pl.ds(pl.multiple_of(HALO + i * tokens, 16), tokens)
    for p, ref in enumerate(pieces):
        cut = pl.ds(pl.multiple_of(order_ref[p] * cols, 128), cols)
        done = (ref[...].astype(F32) * scale * gain_ref[0:1, cut]).astype(BF16)
        out_ref[rows, cut] = done
        send_ref[:, cut] = done[tokens - HALO :, :]


def mixer_kernel(
    order_ref,
    x_ref,
    near_ref,
    far_ref,
    taps_ref,
    wg_ref,
    wv_ref,
    w_ref,
    h_ref,
    far_swap_ref,
    swap_ref,
    own_ref,
    gate_scr,
    value_scr,
    tail_scr,
    x_scr,
    wt_scr,
    down_scr,
    sems,
):
    tokens = near_ref.shape[0]
    tiles, _, tile = taps_ref.shape
    tiles -= 1
    main = tiles * tile
    pairs, cols = down_scr.shape[0], down_scr.shape[1] // 2
    j = pl.program_id(0)

    def copies(n):
        rows = pl.ds(pl.multiple_of(order_ref[n] * cols, 128), cols)
        spot = down_scr.at[n // 2, pl.ds(n % 2 * cols, cols)]
        return (
            pltpu.make_async_copy(
                w_ref.at[rows, pl.ds(2 * main, main)],
                spot.at[:, pl.ds(0, main)],
                sems.at[2 * n],
            ),
            pltpu.make_async_copy(
                w_ref.at[rows, pl.ds(3 * main, 128)],
                spot.at[:, pl.ds(main, 128)],
                sems.at[2 * n + 1],
            ),
        )

    depth = x_scr.shape[1] // 4
    x_cuts = [pl.ds(k * depth, depth) for k in range(4)]
    x_copies = [
        pltpu.make_async_copy(x_ref.at[:, cut], x_scr.at[:, cut], sems.at[8 + k])
        for k, cut in enumerate(x_cuts)
    ]
    wt_copy = pltpu.make_async_copy(w_ref.at[:, pl.ds(3 * main, 128)], wt_scr, sems.at[12])

    def hidden(gate, value, taps, rows):
        near, far = near_ref[rows, :], far_ref[rows, :]
        one = pltpu.roll(gate, 1, 0)[HALO:, :]
        two = pltpu.roll(gate, 2, 0)[HALO:, :]
        conv = (
            taps[2:3, :] * gate[HALO:, :]
            + taps[1:2, :] * (near * one)
            + taps[0:1, :] * (far * two)
        )
        scaled = 0.5 * conv
        return (scaled + scaled * jnp.tanh(scaled)) * value

    block = 96

    def finish(slot, at):
        for start in range(0, tokens, block):
            for half in range(0, tile, 128):
                lanes = slice(half, half + 128)
                done = hidden(
                    gate_scr[slot, start : start + block + HALO, lanes],
                    value_scr[slot, start + HALO : start + HALO + block, lanes],
                    taps_ref[at, :, lanes],
                    slice(start, start + block),
                )
                spot = at * tile + half
                if not isinstance(at, int):
                    spot = pl.multiple_of(spot, 128)
                h_ref[start : start + block, pl.ds(spot, 128)] = done.astype(BF16)

    def finish_tail():
        for start in range(0, tokens, block):
            part = tail_scr[start : start + block + HALO, :]
            lane = lax.broadcasted_iota(jnp.int32, (block, 128), 1)
            mine = (lane >= 64) & (lane < 96)
            done = hidden(
                pltpu.roll(part, 64, 1),
                pltpu.roll(part, 32, 1)[HALO:, :],
                taps_ref[tiles, :, 0:128],
                slice(start, start + block),
            )
            h_ref[start : start + block, main:] = jnp.where(mine, done, 0.0).astype(BF16)

    def project(slot):
        gate_scr[slot] = jnp.dot(x_scr[...], wg_ref[...], preferred_element_type=F32)
        value_scr[slot] = jnp.dot(x_scr[...], wv_ref[...], preferred_element_type=F32)

    def product(n, cuts):
        total = None
        for cut in cuts:
            term = lax.dot_general(
                h_ref[:, cut],
                down_scr[n, :, cut],
                (((1,), (1,)), ((), ())),
                preferred_element_type=F32,
            )
            total = term if total is None else total + term
        return total.astype(BF16)

    @pl.when(j == 0)
    def _():
        for copy in (*x_copies, wt_copy):
            copy.start()
        for n in range(2 * pairs):
            for copy in copies(n):
                copy.start()
        gate = value = None
        for cut, copy in zip(x_cuts, x_copies):
            copy.wait()
            x = x_scr[:, cut]
            gate_part = jnp.dot(x, wg_ref[cut, :], preferred_element_type=F32)
            value_part = jnp.dot(x, wv_ref[cut, :], preferred_element_type=F32)
            gate = gate_part if gate is None else gate + gate_part
            value = value_part if value is None else value + value_part
        gate_scr[0] = gate
        value_scr[0] = value

    @pl.when(j == 1)
    def _():
        wt_copy.wait()
        tail_scr[...] = jnp.dot(x_scr[...], wt_scr[...], preferred_element_type=F32)
        project(1)
        finish_tail()
        finish(0, 0)

    @pl.when((j > 1) & (j < tiles))
    def _():
        project(j % 2)
        finish((j - 1) % 2, j - 1)

    @pl.when(j == tiles)
    def _():
        finish((tiles - 1) % 2, tiles - 1)
        for n in range(2):
            for copy in copies(n):
                copy.wait()
        known = main - tile
        both = product(0, (slice(0, known), slice(main, main + 128), slice(known, main)))
        far_swap_ref[0], own_ref[0] = both[:, :cols], both[:, cols:]

    @pl.when(j > tiles)
    def _():
        for n in range(2, 4):
            for copy in copies(n):
                copy.wait()
        both = product(1, (slice(None),))
        swap_ref[0], swap_ref[1] = both[:, :cols], both[:, cols:]


def two_parts(h_ref, wa_ref, wb_ref, ta_ref, tb_ref):
    main = wa_ref.shape[1]
    contract = (((1,), (1,)), ((), ()))
    main_w = jnp.concatenate([wa_ref[...], wb_ref[...]], axis=0)
    tail_w = jnp.concatenate([ta_ref[...], tb_ref[...]], axis=0)
    both = lax.dot_general(
        h_ref[:, :main], main_w, contract, preferred_element_type=F32
    ) + lax.dot_general(h_ref[:, main:], tail_w, contract, preferred_element_type=F32)
    cols = wa_ref.shape[0]
    return both[:, :cols], both[:, cols:]


def side_kernel(order_ref, h_ref, wa_ref, wb_ref, ta_ref, tb_ref, a_ref, b_ref, up_ref, down_ref):
    up, down = two_parts(h_ref, wa_ref, wb_ref, ta_ref, tb_ref)
    up_ref[...] = (up + a_ref[0].astype(F32)).astype(BF16)
    down_ref[...] = (down + b_ref[0].astype(F32)).astype(BF16)


def down_kernel(order_ref, h_ref, wa_ref, wb_ref, ta_ref, tb_ref, swap_ref, own_ref):
    swap, own = two_parts(h_ref, wa_ref, wb_ref, ta_ref, tb_ref)
    swap_ref[...] = swap.astype(BF16)
    own_ref[...] = own.astype(BF16)


def added(*terms):
    total = terms[0].astype(F32)
    for term in terms[1:]:
        total = total + term.astype(F32)
    return total


def shifted(value, by):
    ring = lax.axis_size("y")
    return lax.ppermute(value, "y", [(i, (i + by) % ring) for i in range(ring)])


def swapped(value):
    return lax.ppermute(value, "c", [(0, 1), (1, 0)])


def summed_over_tp(far_swap, swap, own, sides, last):
    far_swap = swapped(far_swap)
    other = swapped(swap)
    far = added(own, far_swap).astype(BF16)
    half = far.shape[0] // 2
    far_up, far_down = shifted(far[:half], 1), shifted(far[half:], -1)
    up, down = sides(other)
    below, above = shifted(up[half:], 1), shifted(down[:half], -1)
    up = added(up[:half], far_up).astype(BF16)
    down = added(down[half:], far_down).astype(BF16)
    up, down = shifted(up, 1), shifted(down, -1)
    swap, own = last()
    near = added(own, swapped(swap))
    return added(near[:half], up, above), added(near[half:], below, down)


def gathered_over_tp(own):
    half = own.shape[0] // 2
    below, above = shifted(own, 1), shifted(own, -1)
    far = jnp.concatenate([shifted(below[:half], 1), shifted(above[half:], -1)], axis=0)
    mine = [own, below, above, far]
    return mine + [swapped(part) for part in mine]


def shape(dims, dtype):
    return jax.ShapeDtypeStruct(dims, dtype)


def whole(dims):
    return pl.BlockSpec(dims, lambda *_: (0,) * len(dims))


def layer(
    resid,
    query,
    keys,
    values,
    out_gate,
    in_gate,
    forget,
    doc_ids,
    head_gain,
    w_out,
    ffn_gain,
    w_gate,
    w_value,
    conv_taps,
    w_down,
):
    tokens, width = query.shape
    cols = resid.shape[1]
    model = w_out.shape[1]
    hidden = w_gate.shape[1]
    main = hidden // 128 * 128
    spare = hidden - main
    packed = pl.pallas_call(
        pack_kernel,
        in_specs=[pl.BlockSpec(memory_space=pl.ANY)] * 3,
        out_specs=pl.BlockSpec(memory_space=pl.ANY),
        out_shape=shape((w_gate.shape[0], 3 * main + 128), BF16),
        scratch_shapes=[
            pltpu.VMEM((3, w_gate.shape[0], spare), BF16),
            pltpu.VMEM((w_gate.shape[0], 128), BF16),
            pltpu.SemaphoreType.DMA((7,)),
        ],
        name="pack",
    )(w_gate, w_value, w_down.T)
    weights = lax.all_gather(packed, SP, axis=0, tiled=True)
    tile = 256
    tiles = main // tile
    spot = 2 * spare
    taps = jnp.concatenate(
        [
            jnp.swapaxes(conv_taps[:, :main].reshape(3, tiles, tile), 0, 1),
            jnp.pad(conv_taps[:, main:], ((0, 0), (spot, tile - spot - spare)))[None],
        ],
        axis=0,
    )

    pay, rows, cols_aux = pl.pallas_call(
        state_kernel,
        out_shape=(
            shape((DH + 16, width), BF16),
            shape((8, tokens), F32),
            shape((tokens, 8), F32),
        ),
        scratch_shapes=[pltpu.VMEM((8, tokens), F32)],
        name="state",
    )(keys, values, in_gate, forget, doc_ids.reshape(1, tokens))
    count = lax.axis_size(SP)
    reach = -(-(DOC_MAX - 1) // tokens)
    pays = [
        lax.ppermute(pay, SP, [(i, i + k) for i in range(count - k)]) for k in range(1, reach + 1)
    ]
    local = pl.pallas_call(
        local_kernel,
        out_shape=shape((tokens, width), F32),
        name="local",
    )(query, keys, values, rows, cols_aux)
    chip, core = lax.axis_index("y"), lax.axis_index("c")
    ring, cores = lax.axis_size("y"), lax.axis_size("c")
    order = (chip + jnp.array([2, 2, 1, 1, 3, 3, 0, 0], jnp.int32)) % ring * cores + (
        core ^ jnp.array([1, 0] * ring, jnp.int32)
    )
    swap, own, near, far_flags = pl.pallas_call(
        mix_kernel,
        grid_spec=pltpu.PrefetchScalarGridSpec(
            num_scalar_prefetch=1,
            grid=(ring,),
            in_specs=[
                whole((tokens, width)),
                whole((tokens, width)),
                whole((tokens, width)),
                whole((8, tokens)),
                whole((tokens, 8)),
                whole((1, width)),
                pl.BlockSpec((width, cols), lambda j, order: (0, order[2 * j])),
                pl.BlockSpec((width, cols), lambda j, order: (0, order[2 * j + 1])),
                *[whole((DH + 16, width)) for _ in pays],
            ],
            out_specs=(
                pl.BlockSpec((1, tokens, cols), lambda j, order: (j, 0, 0)),
                pl.BlockSpec((1, tokens, cols), lambda j, order: (j, 0, 0)),
                whole((tokens, 128)),
                whole((tokens, 128)),
            ),
            scratch_shapes=[pltpu.VMEM((tokens, width), BF16)],
        ),
        out_shape=(
            shape((ring, tokens, cols), BF16),
            shape((ring, tokens, cols), BF16),
            shape((tokens, 128), F32),
            shape((tokens, 128), F32),
        ),
        name="mix",
    )(order, query, out_gate, local, rows, cols_aux, head_gain.reshape(1, width), w_out, w_out, *pays)
    attended = summed_over_tp(
        swap[0],
        swap[1:3],
        own[0],
        lambda other: tuple(added(own[1 + k], other[k]).astype(BF16) for k in range(2)),
        lambda: (swap[3], own[3]),
    )
    residual_own = resid.astype(F32) + jnp.concatenate(attended, axis=0)
    pieces = gathered_over_tp(residual_own.astype(BF16))
    places = (chip + jnp.array([0, ring - 1, 1, 2] * 2, jnp.int32)) % ring * cores + (
        core ^ jnp.array([0] * ring + [1] * ring, jnp.int32)
    )
    block = 96
    normed, send = pl.pallas_call(
        norm_kernel,
        grid_spec=pltpu.PrefetchScalarGridSpec(
            num_scalar_prefetch=1,
            grid=(tokens // block,),
            in_specs=[
                *[pl.BlockSpec((block, cols), lambda i, places: (i, 0)) for _ in pieces],
                whole((1, model)),
            ],
            out_specs=(whole((tokens + HALO, model)), whole((HALO, model))),
        ),
        out_shape=(shape((tokens + HALO, model), BF16), shape((HALO, model), BF16)),
        compiler_params=pltpu.CompilerParams(vmem_limit_bytes=40 * 2**20),
        name="norm",
    )(places, *pieces, ffn_gain.reshape(1, model))
    edge = lax.ppermute(send, SP, [(i, i + 1) for i in range(count - 1)])
    normed = lax.dynamic_update_slice(normed, edge, (0, 0))
    tail_at = 3 * main // 128
    order = (chip + jnp.array([2, 2, 1, 3, 1, 3, 0, 0], jnp.int32)) % ring * cores + (
        core ^ jnp.array([1, 0, 1, 1, 0, 0, 1, 0], jnp.int32)
    )
    hidden, far_swap, swap, own = pl.pallas_call(
        mixer_kernel,
        grid_spec=pltpu.PrefetchScalarGridSpec(
            num_scalar_prefetch=1,
            grid=(tiles + 2,),
            in_specs=[
                pl.BlockSpec(memory_space=pl.ANY),
                whole((tokens, 128)),
                whole((tokens, 128)),
                whole((tiles + 1, 3, tile)),
                pl.BlockSpec((model, tile), lambda j, order: (0, jnp.minimum(j, tiles - 1))),
                pl.BlockSpec(
                    (model, tile), lambda j, order: (0, tiles + jnp.minimum(j, tiles - 1))
                ),
                pl.BlockSpec(memory_space=pl.ANY),
            ],
            out_specs=(
                whole((tokens, main + 128)),
                whole((1, tokens, cols)),
                whole((2, tokens, cols)),
                whole((1, tokens, cols)),
            ),
            scratch_shapes=[
                pltpu.VMEM((2, tokens + HALO, tile), F32),
                pltpu.VMEM((2, tokens + HALO, tile), F32),
                pltpu.VMEM((tokens + HALO, 128), F32),
                pltpu.VMEM((tokens + HALO, model), BF16),
                pltpu.VMEM((model, 128), BF16),
                pltpu.VMEM((2, 2 * cols, main + 128), BF16),
                pltpu.SemaphoreType.DMA((13,)),
            ],
        ),
        out_shape=(
            shape((tokens, main + 128), BF16),
            shape((1, tokens, cols), BF16),
            shape((2, tokens, cols), BF16),
            shape((1, tokens, cols), BF16),
        ),
        compiler_params=pltpu.CompilerParams(vmem_limit_bytes=58 * 2**20),
        name="mixer",
    )(order, normed, near, far_flags, taps, *[weights] * 3)

    def more(kernel, at, given, specs):
        def spot(k, col):
            return lambda j, order: (order[at + k], col)

        one = shape((tokens, cols), BF16)
        return pl.pallas_call(
            kernel,
            grid_spec=pltpu.PrefetchScalarGridSpec(
                num_scalar_prefetch=1,
                grid=(1,),
                in_specs=[
                    whole((tokens, main + 128)),
                    pl.BlockSpec((cols, main), spot(0, 2)),
                    pl.BlockSpec((cols, main), spot(1, 2)),
                    pl.BlockSpec((cols, 128), spot(0, tail_at)),
                    pl.BlockSpec((cols, 128), spot(1, tail_at)),
                    *specs,
                ],
                out_specs=(whole((tokens, cols)), whole((tokens, cols))),
            ),
            out_shape=(one, one),
            compiler_params=pltpu.CompilerParams(vmem_limit_bytes=40 * 2**20),
        )(order, hidden, *[weights] * 4, *given)

    down = summed_over_tp(
        far_swap[0],
        swap,
        own[0],
        lambda other: more(
            side_kernel,
            4,
            (other, other),
            [pl.BlockSpec((1, tokens, cols), lambda j, order, k=k: (k, 0, 0)) for k in (0, 1)],
        ),
        lambda: more(down_kernel, 6, (), []),
    )
    return (residual_own + jnp.concatenate(down, axis=0)).astype(BF16)


def solution(mesh):
    torus = Mesh(mesh.devices.reshape(4, 4, 4, 2), ("z", "x", "y", "c"))
    placed = (
        P(SP, TP),
        P(SP, TP),
        P(SP, TP),
        P(SP, TP),
        P(SP, TP),
        P(TP, SP),
        P(TP, SP),
        P(SP),
        P(TP),
        P(TP, None),
        P(),
        P(SP, TP),
        P(SP, TP),
        P(None, TP),
        P(TP, SP),
    )
    return jax.shard_map(layer, mesh=torus, in_specs=placed, out_specs=P(SP, TP), check_vma=False)
```

```python
import jax
import jax.numpy as jnp
from jax import lax
from jax.experimental import pallas as pl
from jax.experimental.pallas import tpu as pltpu
from jax.sharding import Mesh
from jax.sharding import PartitionSpec as P


DH = 96
DOC_MAX = 3072
SP = ("z", "x")
TP = ("y", "c")
ABSENT = -1e30
HALO = 16
EPS = 1e-06
HEAD_FLOOR = 1.0
F32 = jnp.float32
BF16 = jnp.bfloat16


def in_first_head(shape):
    return lax.broadcasted_iota(jnp.int32, shape, len(shape) - 1) < DH


def pack_kernel(gate_ref, value_ref, down_ref, out_ref):
    rows, hidden = gate_ref.shape
    main = hidden // 128 * 128
    tails = []
    for k, ref in enumerate((gate_ref, value_ref, down_ref)):
        out_ref[:, k * main : (k + 1) * main] = ref[:, :main]
        tails.append(ref[:, main:])
    tails.append(jnp.zeros((rows, 128 - 3 * (hidden - main)), BF16))
    out_ref[:, 3 * main :] = jnp.concatenate(tails, axis=1)


def state_kernel(k_ref, v_ref, in_ref, forget_ref, doc_ref, pay_ref, row_ref, col_ref, scr):
    tokens, width = k_ref.shape
    lane = lax.broadcasted_iota(jnp.int32, (8, tokens), 1)
    doc = jnp.broadcast_to(doc_ref[...].astype(F32), (8, tokens))
    scr[...] = jnp.zeros_like(scr)
    scr[0:2, :] = forget_ref[...]
    raw = scr[...]
    total = jnp.minimum(raw, 0.0) - jnp.log1p(jnp.exp(-jnp.abs(raw)))
    step = 1
    while step < tokens:
        total = total + jnp.where(lane >= step, pltpu.roll(total, step, 1), 0.0)
        step *= 2
    scr[0:2, :] = in_ref[...]
    rest = scr[...] - total
    peak = rest
    step = 1
    while step < tokens:
        near = (lane >= step) & (pltpu.roll(doc, step, 1) == doc)
        peak = jnp.maximum(peak, jnp.where(near, pltpu.roll(peak, step, 1), ABSENT))
        step *= 2
    end_doc = doc[:, tokens - 1 : tokens]
    end_peak = peak[:, tokens - 1 : tokens]
    end_total = total[:, tokens - 1 : tokens]
    weight = jnp.where(doc == end_doc, jnp.exp(jnp.minimum(rest - end_peak, 0.0)), 0.0)
    row_ref[...] = jnp.zeros_like(row_ref)
    row_ref[0:2, :] = total[0:2, :]
    row_ref[2:4, :] = peak[0:2, :]
    row_ref[4:6, :] = weight[0:2, :]
    row_ref[6:7, :] = doc[0:1, :]
    scr[...] = row_ref[...]
    cols = scr[...].T
    col_ref[...] = cols
    row_ref[4:6, :] = rest[0:2, :]
    first = in_first_head((tokens, width))
    spread = jnp.where(first, cols[:, 4:5], cols[:, 5:6])
    weighted = (k_ref[...].astype(F32) * (spread * DH**-0.5)).astype(BF16)
    state = lax.dot_general(
        weighted, v_ref[...], (((0,), (0,)), ((), ())), preferred_element_type=F32
    )
    small = in_first_head((DH, width))
    pay_ref[0:DH, :] = jnp.where(small, state[0:DH, :], state[DH:, :]).astype(BF16)

    line = in_first_head((1, width))

    def spread_heads(x):
        return jnp.where(line, x[0:1, :], x[1:2, :])

    def split(x):
        high = x.astype(BF16).astype(F32)
        mid = (x - high).astype(BF16).astype(F32)
        return high, mid, x - high - mid

    lines = [
        *split(spread_heads(end_total + end_peak)),
        *split(spread_heads(end_total)),
        jnp.broadcast_to(end_doc[0:1, :] + 1.0, (1, width)),
        jnp.broadcast_to(doc[0:1, tokens - 2 : tokens - 1] + 1.0, (1, width)),
    ]
    place = lax.broadcasted_iota(jnp.int32, (16, width), 0)
    table = jnp.zeros((16, width), F32)
    for k, value in enumerate(lines):
        table = jnp.where(place == k, value, table)
    pay_ref[DH:, :] = table.astype(BF16)


def local_kernel(q_ref, k_ref, v_ref, row_ref, col_ref, out_ref):
    tokens, width = q_ref.shape
    block = 256
    for start in range(0, tokens, block):
        stop = start + block
        keys = k_ref[0:stop, :]
        vals = v_ref[0:stop, :]
        q = q_ref[start:stop, :]
        first = in_first_head((block, width))
        at = lax.broadcasted_iota(jnp.int32, (block, stop), 0) + start
        source = lax.broadcasted_iota(jnp.int32, (block, stop), 1)
        seen = (at >= source) & (row_ref[6:7, 0:stop] == col_ref[start:stop, 6:7])
        found = []
        for h in range(2):
            mine = jnp.where(first if h == 0 else jnp.logical_not(first), q, jnp.zeros_like(q))
            scores = lax.dot_general(
                mine, keys, (((1,), (1,)), ((), ())), preferred_element_type=F32
            )
            gap = row_ref[4 + h : 5 + h, 0:stop] - col_ref[start:stop, 2 + h : 3 + h]
            part = (scores * jnp.exp(jnp.where(seen, gap, ABSENT))).astype(BF16)
            found.append(jnp.dot(part, vals, preferred_element_type=F32))
        out_ref[start:stop, :] = jnp.where(first, found[0], found[1])


def mix_kernel(
    order_ref, q_ref, gate_ref, local_ref, row_ref, col_ref, gain_ref, w_ref, *refs
):
    w_own_ref, *pays = refs[:-5]
    swap_ref, own_out_ref, near_ref, far_ref, mix_ref = refs[-5:]
    tokens, width = q_ref.shape

    @pl.when(pl.program_id(0) == 0)
    def _():
        own = row_ref[6:7, 0:1] + 1.0
        behind = jnp.zeros((1, width), F32)
        peaks, goods = [], []
        for ref in pays:
            table = ref[DH:, :].astype(F32)
            good = table[6:7, :] == own
            peaks.append(
                jnp.where(good, table[0:1, :] + table[1:2, :] + table[2:3, :] + behind, ABSENT)
            )
            goods.append(good)
            behind = behind + (table[3:4, :] + table[4:5, :] + table[5:6, :])
        best = peaks[0]
        for value in peaks[1:]:
            best = jnp.maximum(best, value)
        state = jnp.zeros((DH, width), F32)
        for ref, value, good in zip(pays, peaks, goods):
            state = state + jnp.where(good, jnp.exp(value - best), 0.0) * ref[0:DH, :].astype(F32)
        small = in_first_head((DH, width))
        whole = jnp.concatenate(
            [jnp.where(small, state, 0.0), jnp.where(small, 0.0, state)], axis=0
        ).astype(BF16)
        carried = jnp.dot(q_ref[...], whole, preferred_element_type=F32)
        first = in_first_head((tokens, width))
        total = jnp.where(first, col_ref[:, 0:1], col_ref[:, 1:2])
        peak = total + jnp.where(first, col_ref[:, 2:3], col_ref[:, 3:4])
        inter = jnp.where(col_ref[:, 6:7] + 1.0 == own, total + best, ABSENT)
        top = jnp.maximum(peak, inter)
        memory = (
            jnp.exp(peak - top) * (local_ref[...] * DH**-0.5) + jnp.exp(inter - top) * carried
        )
        square = memory * memory
        mean_0 = jnp.sum(jnp.where(first, square, 0.0), axis=1, keepdims=True) / DH
        mean_1 = jnp.sum(jnp.where(first, 0.0, square), axis=1, keepdims=True) / DH
        norm = jnp.where(first, lax.rsqrt(mean_0 + HEAD_FLOOR), lax.rsqrt(mean_1 + HEAD_FLOOR))
        gate = gate_ref[...].astype(F32)
        mix_ref[...] = (memory * norm * gain_ref[...] * (1.0 / (1.0 + jnp.exp(-gate)))).astype(BF16)

        ids = pays[0][DH:, :].astype(F32)
        last, second = ids[6:7, 0:1], ids[7:8, 0:1]
        doc = jnp.broadcast_to(col_ref[:, 6:7], (tokens, 128)) + 1.0
        row = lax.broadcasted_iota(jnp.int32, (tokens, 128), 0)
        one = jnp.where(row == 0, last, pltpu.roll(doc, 1, 0))
        two = jnp.where(row == 0, second, jnp.where(row == 1, last, pltpu.roll(doc, 2, 0)))
        near_ref[...] = (one == doc).astype(F32)
        far_ref[...] = (two == doc).astype(F32)

    mix = mix_ref[...]
    swap_ref[0] = jnp.dot(mix, w_ref[...], preferred_element_type=F32).astype(BF16)
    own_out_ref[0] = jnp.dot(mix, w_own_ref[...], preferred_element_type=F32).astype(BF16)


def norm_kernel(order_ref, *refs):
    pieces, (gain_ref, out_ref, send_ref) = refs[:-3], refs[-3:]
    tokens, cols = pieces[0].shape
    model = out_ref.shape[1]
    i = pl.program_id(0)
    square = jnp.zeros((tokens, cols), F32)
    for ref in pieces:
        r = ref[...].astype(F32)
        square = square + r * r
    mean = jnp.sum(square, axis=1, keepdims=True) / model
    scale = lax.rsqrt(mean + EPS)
    rows = pl.ds(pl.multiple_of(HALO + i * tokens, 16), tokens)
    for p, ref in enumerate(pieces):
        cut = pl.ds(pl.multiple_of(order_ref[p] * cols, 128), cols)
        done = (ref[...].astype(F32) * scale * gain_ref[0:1, cut]).astype(BF16)
        out_ref[rows, cut] = done
        send_ref[:, cut] = done[tokens - HALO :, :]


def mixer_kernel(
    order_ref,
    x_ref,
    near_ref,
    far_ref,
    taps_ref,
    wg_ref,
    wv_ref,
    wt_ref,
    w_ref,
    h_ref,
    far_swap_ref,
    swap_ref,
    own_ref,
    gate_scr,
    value_scr,
    tail_scr,
    down_scr,
    sems,
):
    tokens = near_ref.shape[0]
    tiles, _, tile = taps_ref.shape
    tiles -= 1
    main = tiles * tile
    pairs, cols = down_scr.shape[0], down_scr.shape[1] // 2
    j = pl.program_id(0)

    def copies(n):
        rows = pl.ds(pl.multiple_of(order_ref[n] * cols, 128), cols)
        spot = down_scr.at[n // 2, pl.ds(n % 2 * cols, cols)]
        return (
            pltpu.make_async_copy(
                w_ref.at[rows, pl.ds(2 * main, main)],
                spot.at[:, pl.ds(0, main)],
                sems.at[2 * n],
            ),
            pltpu.make_async_copy(
                w_ref.at[rows, pl.ds(3 * main, 128)],
                spot.at[:, pl.ds(main, 128)],
                sems.at[2 * n + 1],
            ),
        )

    def hidden(gate, value, taps, rows):
        near, far = near_ref[rows, :], far_ref[rows, :]
        one = pltpu.roll(gate, 1, 0)[HALO:, :]
        two = pltpu.roll(gate, 2, 0)[HALO:, :]
        conv = (
            taps[2:3, :] * gate[HALO:, :]
            + taps[1:2, :] * (near * one)
            + taps[0:1, :] * (far * two)
        )
        scaled = 0.5 * conv
        return (scaled + scaled * jnp.tanh(scaled)) * value

    block = 96

    def finish(slot, at):
        for start in range(0, tokens, block):
            for half in range(0, tile, 128):
                lanes = slice(half, half + 128)
                done = hidden(
                    gate_scr[slot, start : start + block + HALO, lanes],
                    value_scr[slot, start + HALO : start + HALO + block, lanes],
                    taps_ref[at, :, lanes],
                    slice(start, start + block),
                )
                spot = at * tile + half
                if not isinstance(at, int):
                    spot = pl.multiple_of(spot, 128)
                h_ref[start : start + block, pl.ds(spot, 128)] = done.astype(BF16)

    def finish_tail():
        for start in range(0, tokens, block):
            part = tail_scr[start : start + block + HALO, :]
            lane = lax.broadcasted_iota(jnp.int32, (block, 128), 1)
            mine = (lane >= 64) & (lane < 96)
            done = hidden(
                pltpu.roll(part, 64, 1),
                pltpu.roll(part, 32, 1)[HALO:, :],
                taps_ref[tiles, :, 0:128],
                slice(start, start + block),
            )
            h_ref[start : start + block, main:] = jnp.where(mine, done, 0.0).astype(BF16)

    def project(slot):
        gate_scr[slot] = jnp.dot(x_ref[...], wg_ref[...], preferred_element_type=F32)
        value_scr[slot] = jnp.dot(x_ref[...], wv_ref[...], preferred_element_type=F32)

    def product(n, cuts):
        total = None
        for cut in cuts:
            term = lax.dot_general(
                h_ref[:, cut],
                down_scr[n, :, cut],
                (((1,), (1,)), ((), ())),
                preferred_element_type=F32,
            )
            total = term if total is None else total + term
        return total.astype(BF16)

    @pl.when(j == 0)
    def _():
        for n in range(2 * pairs):
            for copy in copies(n):
                copy.start()
        tail_scr[...] = jnp.dot(x_ref[...], wt_ref[...], preferred_element_type=F32)
        project(0)

    @pl.when(j == 1)
    def _():
        project(1)
        finish_tail()
        finish(0, 0)

    @pl.when((j > 1) & (j < tiles))
    def _():
        project(j % 2)
        finish((j - 1) % 2, j - 1)

    @pl.when(j == tiles)
    def _():
        finish((tiles - 1) % 2, tiles - 1)
        for n in range(2):
            for copy in copies(n):
                copy.wait()
        known = main - tile
        both = product(0, (slice(0, known), slice(main, main + 128), slice(known, main)))
        far_swap_ref[0], own_ref[0] = both[:, :cols], both[:, cols:]

    @pl.when(j > tiles)
    def _():
        for n in range(2, 4):
            for copy in copies(n):
                copy.wait()
        both = product(1, (slice(None),))
        swap_ref[0], swap_ref[1] = both[:, :cols], both[:, cols:]


def two_parts(h_ref, wa_ref, wb_ref, ta_ref, tb_ref):
    main = wa_ref.shape[1]
    contract = (((1,), (1,)), ((), ()))
    main_w = jnp.concatenate([wa_ref[...], wb_ref[...]], axis=0)
    tail_w = jnp.concatenate([ta_ref[...], tb_ref[...]], axis=0)
    both = lax.dot_general(
        h_ref[:, :main], main_w, contract, preferred_element_type=F32
    ) + lax.dot_general(h_ref[:, main:], tail_w, contract, preferred_element_type=F32)
    cols = wa_ref.shape[0]
    return both[:, :cols], both[:, cols:]


def side_kernel(order_ref, h_ref, wa_ref, wb_ref, ta_ref, tb_ref, a_ref, b_ref, up_ref, down_ref):
    up, down = two_parts(h_ref, wa_ref, wb_ref, ta_ref, tb_ref)
    up_ref[...] = (up + a_ref[0].astype(F32)).astype(BF16)
    down_ref[...] = (down + b_ref[0].astype(F32)).astype(BF16)


def down_kernel(order_ref, h_ref, wa_ref, wb_ref, ta_ref, tb_ref, swap_ref, own_ref):
    swap, own = two_parts(h_ref, wa_ref, wb_ref, ta_ref, tb_ref)
    swap_ref[...] = swap.astype(BF16)
    own_ref[...] = own.astype(BF16)


def added(*terms):
    total = terms[0].astype(F32)
    for term in terms[1:]:
        total = total + term.astype(F32)
    return total


def shifted(value, by):
    ring = lax.axis_size("y")
    return lax.ppermute(value, "y", [(i, (i + by) % ring) for i in range(ring)])


def swapped(value):
    return lax.ppermute(value, "c", [(0, 1), (1, 0)])


def summed_over_tp(far_swap, swap, own, sides, last):
    far_swap = swapped(far_swap)
    other = swapped(swap)
    far = added(own, far_swap).astype(BF16)
    half = far.shape[0] // 2
    far_up, far_down = shifted(far[:half], 1), shifted(far[half:], -1)
    up, down = sides(other)
    below, above = shifted(up[half:], 1), shifted(down[:half], -1)
    up = added(up[:half], far_up).astype(BF16)
    down = added(down[half:], far_down).astype(BF16)
    up, down = shifted(up, 1), shifted(down, -1)
    swap, own = last()
    near = added(own, swapped(swap))
    return added(near[:half], up, above), added(near[half:], below, down)


def gathered_over_tp(own):
    half = own.shape[0] // 2
    below, above = shifted(own, 1), shifted(own, -1)
    far = jnp.concatenate([shifted(below[:half], 1), shifted(above[half:], -1)], axis=0)
    mine = [own, below, above, far]
    return mine + [swapped(part) for part in mine]


def shape(dims, dtype):
    return jax.ShapeDtypeStruct(dims, dtype)


def whole(dims):
    return pl.BlockSpec(dims, lambda *_: (0,) * len(dims))


def layer(
    resid,
    query,
    keys,
    values,
    out_gate,
    in_gate,
    forget,
    doc_ids,
    head_gain,
    w_out,
    ffn_gain,
    w_gate,
    w_value,
    conv_taps,
    w_down,
):
    tokens, width = query.shape
    cols = resid.shape[1]
    model = w_out.shape[1]
    hidden = w_gate.shape[1]
    main = hidden // 128 * 128
    spare = hidden - main
    packed = pl.pallas_call(
        pack_kernel,
        grid=(3,),
        in_specs=[pl.BlockSpec((w_gate.shape[0] // 3, hidden), lambda i: (i, 0))] * 3,
        out_specs=pl.BlockSpec((w_gate.shape[0] // 3, 3 * main + 128), lambda i: (i, 0)),
        out_shape=shape((w_gate.shape[0], 3 * main + 128), BF16),
        name="pack",
    )(w_gate, w_value, w_down.T)
    weights = lax.all_gather(packed, SP, axis=0, tiled=True)
    tile = 256
    tiles = main // tile
    spot = 2 * spare
    taps = jnp.concatenate(
        [
            jnp.swapaxes(conv_taps[:, :main].reshape(3, tiles, tile), 0, 1),
            jnp.pad(conv_taps[:, main:], ((0, 0), (spot, tile - spot - spare)))[None],
        ],
        axis=0,
    )

    pay, rows, cols_aux = pl.pallas_call(
        state_kernel,
        out_shape=(
            shape((DH + 16, width), BF16),
            shape((8, tokens), F32),
            shape((tokens, 8), F32),
        ),
        scratch_shapes=[pltpu.VMEM((8, tokens), F32)],
        name="state",
    )(keys, values, in_gate, forget, doc_ids.reshape(1, tokens))
    count = lax.axis_size(SP)
    reach = -(-(DOC_MAX - 1) // tokens)
    pays = [
        lax.ppermute(pay, SP, [(i, i + k) for i in range(count - k)]) for k in range(1, reach + 1)
    ]
    local = pl.pallas_call(
        local_kernel,
        out_shape=shape((tokens, width), F32),
        name="local",
    )(query, keys, values, rows, cols_aux)
    chip, core = lax.axis_index("y"), lax.axis_index("c")
    ring, cores = lax.axis_size("y"), lax.axis_size("c")
    order = (chip + jnp.array([2, 2, 1, 1, 3, 3, 0, 0], jnp.int32)) % ring * cores + (
        core ^ jnp.array([1, 0] * ring, jnp.int32)
    )
    swap, own, near, far_flags = pl.pallas_call(
        mix_kernel,
        grid_spec=pltpu.PrefetchScalarGridSpec(
            num_scalar_prefetch=1,
            grid=(ring,),
            in_specs=[
                whole((tokens, width)),
                whole((tokens, width)),
                whole((tokens, width)),
                whole((8, tokens)),
                whole((tokens, 8)),
                whole((1, width)),
                pl.BlockSpec((width, cols), lambda j, order: (0, order[2 * j])),
                pl.BlockSpec((width, cols), lambda j, order: (0, order[2 * j + 1])),
                *[whole((DH + 16, width)) for _ in pays],
            ],
            out_specs=(
                pl.BlockSpec((1, tokens, cols), lambda j, order: (j, 0, 0)),
                pl.BlockSpec((1, tokens, cols), lambda j, order: (j, 0, 0)),
                whole((tokens, 128)),
                whole((tokens, 128)),
            ),
            scratch_shapes=[pltpu.VMEM((tokens, width), BF16)],
        ),
        out_shape=(
            shape((ring, tokens, cols), BF16),
            shape((ring, tokens, cols), BF16),
            shape((tokens, 128), F32),
            shape((tokens, 128), F32),
        ),
        name="mix",
    )(order, query, out_gate, local, rows, cols_aux, head_gain.reshape(1, width), w_out, w_out, *pays)
    attended = summed_over_tp(
        swap[0],
        swap[1:3],
        own[0],
        lambda other: tuple(added(own[1 + k], other[k]).astype(BF16) for k in range(2)),
        lambda: (swap[3], own[3]),
    )
    residual_own = resid.astype(F32) + jnp.concatenate(attended, axis=0)
    pieces = gathered_over_tp(residual_own.astype(BF16))
    places = (chip + jnp.array([0, ring - 1, 1, 2] * 2, jnp.int32)) % ring * cores + (
        core ^ jnp.array([0] * ring + [1] * ring, jnp.int32)
    )
    block = 96
    normed, send = pl.pallas_call(
        norm_kernel,
        grid_spec=pltpu.PrefetchScalarGridSpec(
            num_scalar_prefetch=1,
            grid=(tokens // block,),
            in_specs=[
                *[pl.BlockSpec((block, cols), lambda i, places: (i, 0)) for _ in pieces],
                whole((1, model)),
            ],
            out_specs=(whole((tokens + HALO, model)), whole((HALO, model))),
        ),
        out_shape=(shape((tokens + HALO, model), BF16), shape((HALO, model), BF16)),
        compiler_params=pltpu.CompilerParams(vmem_limit_bytes=40 * 2**20),
        name="norm",
    )(places, *pieces, ffn_gain.reshape(1, model))
    edge = lax.ppermute(send, SP, [(i, i + 1) for i in range(count - 1)])
    normed = lax.dynamic_update_slice(normed, edge, (0, 0))
    tail_at = 3 * main // 128
    order = (chip + jnp.array([2, 2, 1, 3, 1, 3, 0, 0], jnp.int32)) % ring * cores + (
        core ^ jnp.array([1, 0, 1, 1, 0, 0, 1, 0], jnp.int32)
    )
    hidden, far_swap, swap, own = pl.pallas_call(
        mixer_kernel,
        grid_spec=pltpu.PrefetchScalarGridSpec(
            num_scalar_prefetch=1,
            grid=(tiles + 2,),
            in_specs=[
                pl.BlockSpec(
                    (tokens + HALO, model), lambda j, order: (0, 0), pipeline_mode=pl.Buffered(1)
                ),
                whole((tokens, 128)),
                whole((tokens, 128)),
                whole((tiles + 1, 3, tile)),
                pl.BlockSpec((model, tile), lambda j, order: (0, jnp.minimum(j, tiles - 1))),
                pl.BlockSpec(
                    (model, tile), lambda j, order: (0, tiles + jnp.minimum(j, tiles - 1))
                ),
                pl.BlockSpec(
                    (model, 128), lambda j, order: (0, tail_at), pipeline_mode=pl.Buffered(1)
                ),
                pl.BlockSpec(memory_space=pl.ANY),
            ],
            out_specs=(
                whole((tokens, main + 128)),
                whole((1, tokens, cols)),
                whole((2, tokens, cols)),
                whole((1, tokens, cols)),
            ),
            scratch_shapes=[
                pltpu.VMEM((2, tokens + HALO, tile), F32),
                pltpu.VMEM((2, tokens + HALO, tile), F32),
                pltpu.VMEM((tokens + HALO, 128), F32),
                pltpu.VMEM((2, 2 * cols, main + 128), BF16),
                pltpu.SemaphoreType.DMA((8,)),
            ],
        ),
        out_shape=(
            shape((tokens, main + 128), BF16),
            shape((1, tokens, cols), BF16),
            shape((2, tokens, cols), BF16),
            shape((1, tokens, cols), BF16),
        ),
        compiler_params=pltpu.CompilerParams(vmem_limit_bytes=58 * 2**20),
        name="mixer",
    )(order, normed, near, far_flags, taps, *[weights] * 4)

    def more(kernel, at, given, specs):
        def spot(k, col):
            return lambda j, order: (order[at + k], col)

        one = shape((tokens, cols), BF16)
        return pl.pallas_call(
            kernel,
            grid_spec=pltpu.PrefetchScalarGridSpec(
                num_scalar_prefetch=1,
                grid=(1,),
                in_specs=[
                    whole((tokens, main + 128)),
                    pl.BlockSpec((cols, main), spot(0, 2)),
                    pl.BlockSpec((cols, main), spot(1, 2)),
                    pl.BlockSpec((cols, 128), spot(0, tail_at)),
                    pl.BlockSpec((cols, 128), spot(1, tail_at)),
                    *specs,
                ],
                out_specs=(whole((tokens, cols)), whole((tokens, cols))),
            ),
            out_shape=(one, one),
            compiler_params=pltpu.CompilerParams(vmem_limit_bytes=40 * 2**20),
        )(order, hidden, *[weights] * 4, *given)

    down = summed_over_tp(
        far_swap[0],
        swap,
        own[0],
        lambda other: more(
            side_kernel,
            4,
            (other, other),
            [pl.BlockSpec((1, tokens, cols), lambda j, order, k=k: (k, 0, 0)) for k in (0, 1)],
        ),
        lambda: more(down_kernel, 6, (), []),
    )
    return (residual_own + jnp.concatenate(down, axis=0)).astype(BF16)


def solution(mesh):
    torus = Mesh(mesh.devices.reshape(4, 4, 4, 2), ("z", "x", "y", "c"))
    placed = (
        P(SP, TP),
        P(SP, TP),
        P(SP, TP),
        P(SP, TP),
        P(SP, TP),
        P(TP, SP),
        P(TP, SP),
        P(SP),
        P(TP),
        P(TP, None),
        P(),
        P(SP, TP),
        P(SP, TP),
        P(None, TP),
        P(TP, SP),
    )
    return jax.shard_map(layer, mesh=torus, in_specs=placed, out_specs=P(SP, TP), check_vma=False)
```
